512 devices in a mesh: sp: 128 (over z, x, core), tp: 4 (over y).
Axes of the slice: x: 4, y: 4, z: 16, core: 2. Of those that a mesh axis runs over, the one named last changes fastest.
Arguments:
- query_main: bfloat16 [16384, 2048], P('sp', 'tp'), may hold values from -6 to 6
- query_rotary: bfloat16 [16384, 1024], P('sp', 'tp'), may hold values from -7 to 7
- latent: bfloat16 [16384, 512], P('sp'), may hold values from -24 to 24
- key_rotary: bfloat16 [16384, 64], P('sp'), may hold values from -8 to 8
- key_weight: bfloat16 [512, 2048], P(None, 'tp'), may hold values from -0.25 to 0.25
- value_weight: bfloat16 [512, 2048], P(None, 'tp'), may hold values from -0.25 to 0.25
- head_output: bfloat16 [16384, 2048], P('sp', 'tp'), may hold values from -2 to 2
- output_grad: bfloat16 [16384, 2048], P('sp', 'tp'), may hold values from -128 to 128
- row_logsum: float32 [16, 16384], P('tp', 'sp'), may hold values from 3 to 16, as said below
Outputs:
- grad_query_main: float32 [16384, 2048], P('sp', 'tp')
- grad_query_rotary: float32 [16384, 1024], P('sp', 'tp')
- grad_latent: float32 [16384, 512], P('sp')
- grad_key_rotary: float32 [16384, 64], P('sp')
- grad_key_weight: float32 [512, 2048], P('sp', 'tp')
The draws below stay inside these ranges and needn't reach their ends.
Inputs may be any that keep to these rules, and one draw needn't show every extreme that they name: With p the place of token i in its sequence and q = i % 128, row_logsum[h, i] minus the logarithm of (p + 1 + 54 (q + 1)) lies between -0.3 and 1.5.
All inputs are finite; a program needn't handle non-finite values.
Results may differ from the reference program's by a relative error of at most 0.003.
The reference program's roundings to bfloat16 on the way (of `query_latent`, `grad_rows`, `weights_low`, `dscores_low` and `mixed_low`) count: a program that leaves them out, or rounds other values in their place, can miss the bound.
Values may be sent and summed in bfloat16 or wider, within the bound.
A program may use at most 64 MiB of HBM per device.

```python
import math
import jax
import jax.numpy as jnp
from jax import lax

TOK_DEV = 128
HEADS = 16
KDIM = 128
RDIM = 64
VDIM = 128
LATENT = 512
SPAN = 32
LEAD = 8
SEQS = 5
TOKENS = 16384
N_SP = 128


own_mass = 54.0


def block_signs(key):
    picks = jax.random.randint(jax.random.fold_in(key, 7), (TOKENS // TOK_DEV, RDIM), 0, 2)
    table = picks.astype(jnp.float32) * 2.0 - 1.0
    return table[jnp.arange(TOKENS) // TOK_DEV]


def noise_field(key, shape):
    return jnp.clip(jax.random.normal(key, shape, jnp.float32), -6.0, 6.0)


def draw_query_rotary(key, part):
    signs = block_signs(key)
    noise = noise_field(jax.random.fold_in(key, 11), (TOKENS, HEADS, RDIM))
    return (noise + signs[:, None, :]).reshape(TOKENS, HEADS * RDIM).astype(jnp.bfloat16)


def draw_key_rotary(key, part):
    signs = block_signs(key)
    noise = noise_field(jax.random.fold_in(key, 13), (TOKENS, RDIM))
    strength = 4.0 * (KDIM + RDIM) ** 0.5 / RDIM
    return (noise + strength * signs).astype(jnp.bfloat16)


def draw_row_logsum(key, part):
    token = jnp.arange(TOKENS)
    device = token // TOK_DEV
    sequence = (device + LEAD) // SPAN
    first_device = jnp.maximum(sequence * SPAN - LEAD, 0)
    place = (token - first_device * TOK_DEV + 1).astype(jnp.float32)
    inside = (token % TOK_DEV + 1).astype(jnp.float32)
    total = place + own_mass * inside
    offset = jax.random.uniform(key, (HEADS, TOKENS), jnp.float32, 0.2, 1.2)
    return jnp.log(total)[None, :] + offset


def with_spikes(drawn, own_key, source, target, parts, factor):
    def block_of(axis_at):
        return (jnp.arange(drawn.shape[axis_at]) // (drawn.shape[axis_at] // parts)).reshape((-1,) + (1,) * (drawn.ndim - 1 - axis_at))

    near = jax.random.permutation(own_key, parts)[block_of(target)]
    second = (block_of(target) + parts // 2) % parts
    return jnp.where((block_of(source) == near) | (block_of(source) == second), factor * drawn, drawn)


def levels(key, shape, split, smallest, top_value):
    gain = 1.0
    for axis_at, parts in split:
        heights = jax.random.uniform(jax.random.fold_in(jax.random.fold_in(key, 6), axis_at), (parts,), jnp.float32, smallest / len(split), top_value / len(split))
        gain = gain * jnp.repeat(jnp.exp(heights), shape[axis_at] // parts).reshape((-1,) + (1,) * (len(shape) - 1 - axis_at))
    return gain


def centred(stream_key, extent, scale, bound, pieces=(), held_as=jnp.bfloat16):
    entries = jax.random.normal(stream_key, extent, jnp.float32) * scale
    if len(pieces) > 0:
        entries = levels(stream_key, extent, pieces, -0.22, 0.18) * entries
    return jnp.clip(entries, min=-bound, max=bound).astype(held_as)


def noise_with(own_key, shape, spread, most, split, heavy, held_as=jnp.bfloat16):
    entries = spread * jax.random.normal(own_key, shape, jnp.float32)
    if split:
        entries = entries * levels(own_key, shape, split, -0.22, 0.18)
    return jnp.clip(with_spikes(entries, jax.random.fold_in(own_key, 3), *heavy), -most, most).astype(held_as)


def setup_inputs(seed: int = 0) -> dict:
    seeds = jax.random.split(jax.random.key(seed), 10)
    query_main = centred(seeds[0], (TOKENS, HEADS * KDIM), 1.0, 6.0, ((0, 128), (1, 4)))
    query_rotary = draw_query_rotary(jax.random.fold_in(seeds[9], 71), 0)
    latent = noise_with(seeds[2], (TOKENS, LATENT), 1.0, 24.0, ((0, 128),), (0, 1, 128, 5.5))
    key_rotary = draw_key_rotary(jax.random.fold_in(seeds[9], 71), 0)
    key_weight = centred(seeds[4], (LATENT, HEADS * KDIM), LATENT ** -0.5, 0.25, ((1, 4),))
    value_weight = centred(seeds[5], (LATENT, HEADS * VDIM), LATENT ** -0.5, 0.25, ((1, 4),))
    head_output = centred(seeds[6], (TOKENS, HEADS * VDIM), 0.3, 2.0, ((0, 128), (1, 4)))
    output_grad = noise_with(seeds[7], (TOKENS, HEADS * VDIM), 6.0, 128.0, ((0, 128), (1, 4)), (0, 1, 128, 5.5))
    row_logsum = draw_row_logsum(jax.random.fold_in(seeds[9], 71), 0)
    return {"query_main": query_main, "query_rotary": query_rotary, "latent": latent, "key_rotary": key_rotary, "key_weight": key_weight, "value_weight": value_weight, "head_output": head_output, "output_grad": output_grad, "row_logsum": row_logsum}


def sequence_grads(lat_seq, rot_seq, query_latent, grad_rows, rot_query, row_logs, row_terms, factor, width):
    wide = jnp.float32
    blocks = lat_seq.shape[0] // width
    heads = query_latent.shape[1]
    lat_all = lat_seq.astype(wide)
    rot_all = rot_seq.astype(wide)
    qlat_all = query_latent.astype(wide)
    grows_all = grad_rows.astype(wide)
    qrot_all = rot_query.astype(wide)

    def query_block(carry, query_index):
        acc_lat, acc_rot = carry
        query_start = (query_index * width).astype(jnp.int32)
        qlat = lax.dynamic_slice_in_dim(qlat_all, query_start, width, 0)
        grows = lax.dynamic_slice_in_dim(grows_all, query_start, width, 0)
        qrot = lax.dynamic_slice_in_dim(qrot_all, query_start, width, 0)
        logs = lax.dynamic_slice_in_dim(row_logs, query_start, width, 0)
        terms = lax.dynamic_slice_in_dim(row_terms, query_start, width, 0)
        query_place = query_start + jnp.arange(width, dtype=jnp.int32)

        def key_block(key_index, inner):
            def visit(state):
                mixed_sum, rot_sum, acc_lat, acc_rot = state
                key_start = (key_index * width).astype(jnp.int32)
                lat_block = lax.dynamic_slice_in_dim(lat_all, key_start, width, 0)
                rot_block = lax.dynamic_slice_in_dim(rot_all, key_start, width, 0)
                key_place = key_start + jnp.arange(width, dtype=jnp.int32)
                seen = key_place[None, :] <= query_place[:, None]
                scores = jnp.einsum("thl,kl->thk", qlat, lat_block) + jnp.einsum("thr,kr->thk", qrot, rot_block)
                weights = jnp.where(seen[:, None, :], jnp.exp(factor * scores - logs[:, :, None]), 0.0)
                slopes = jnp.einsum("thl,kl->thk", grows, lat_block)
                dscores = weights * (slopes - terms[:, :, None])
                weights_low = lax.optimization_barrier(weights.astype(jnp.bfloat16)).astype(wide)
                dscores_low = lax.optimization_barrier(dscores.astype(jnp.bfloat16)).astype(wide)
                mixed_sum = mixed_sum + jnp.einsum("thk,kl->thl", dscores_low, lat_block)
                rot_sum = rot_sum + jnp.einsum("thk,kr->thr", dscores_low, rot_block)
                part_lat = factor * jnp.einsum("thk,thl->kl", dscores_low, qlat) + jnp.einsum("thk,thl->kl", weights_low, grows)
                part_rot = factor * jnp.einsum("thk,thr->kr", dscores_low, qrot)
                old_lat = lax.dynamic_slice_in_dim(acc_lat, key_start, width, 0)
                old_rot = lax.dynamic_slice_in_dim(acc_rot, key_start, width, 0)
                acc_lat = lax.dynamic_update_slice_in_dim(acc_lat, old_lat + part_lat, key_start, 0)
                acc_rot = lax.dynamic_update_slice_in_dim(acc_rot, old_rot + part_rot, key_start, 0)
                return mixed_sum, rot_sum, acc_lat, acc_rot

            def keep(state):
                return state

            return lax.cond(key_index <= query_index, visit, keep, inner)

        start_state = (jnp.zeros((width, heads, lat_all.shape[1]), wide), jnp.zeros((width, heads, rot_all.shape[1]), wide), acc_lat, acc_rot)
        mixed_sum, rot_sum, acc_lat, acc_rot = lax.fori_loop(0, blocks, key_block, start_state)
        return (acc_lat, acc_rot), (mixed_sum, rot_sum)

    start = (jnp.zeros(lat_seq.shape, wide), jnp.zeros(rot_seq.shape, wide))
    (acc_lat, acc_rot), (mixed_parts, rot_parts) = lax.scan(query_block, start, jnp.arange(blocks, dtype=jnp.int32))
    mixed = mixed_parts.reshape(lat_seq.shape[0], heads, lat_seq.shape[1])
    rot_sum = rot_parts.reshape(lat_seq.shape[0], heads, rot_seq.shape[1])
    return mixed, rot_sum, acc_lat, acc_rot


def reference(query_main, query_rotary, latent, key_rotary, key_weight, value_weight, head_output, output_grad, row_logsum):
    wide = jnp.float32
    factor = (KDIM + RDIM) ** -0.5
    count = latent.shape[0]
    width = math.gcd(LEAD * TOK_DEV, 512)
    main_query = query_main.reshape(count, HEADS, KDIM).astype(wide)
    rot_query = query_rotary.reshape(count, HEADS, RDIM)
    key_proj = key_weight.reshape(LATENT, HEADS, KDIM).astype(wide)
    value_proj = value_weight.reshape(LATENT, HEADS, VDIM).astype(wide)
    grad_heads = output_grad.reshape(count, HEADS, VDIM).astype(wide)
    query_latent = jnp.einsum("thd,lhd->thl", main_query, key_proj).astype(jnp.bfloat16)
    grad_rows = jnp.einsum("thd,lhd->thl", grad_heads, value_proj).astype(jnp.bfloat16)
    row_terms = jnp.sum(head_output.reshape(count, HEADS, VDIM).astype(wide) * grad_heads, axis=2)
    row_logs = row_logsum.T.astype(wide)
    mixed_list, rot_list, lat_list, key_rot_list = [], [], [], []
    for sequence in range(SEQS):
        first = max(sequence * SPAN - LEAD, 0) * TOK_DEV
        last = min((sequence + 1) * SPAN - LEAD, N_SP) * TOK_DEV
        mixed, rot_sum, acc_lat, acc_rot = sequence_grads(
            latent[first:last], key_rotary[first:last], query_latent[first:last], grad_rows[first:last],
            rot_query[first:last], row_logs[first:last], row_terms[first:last], factor, width)
        mixed_list.append(mixed)
        rot_list.append(rot_sum)
        lat_list.append(acc_lat)
        key_rot_list.append(acc_rot)
    mixed = jnp.concatenate(mixed_list, axis=0)
    rot_sum = jnp.concatenate(rot_list, axis=0)
    grad_latent = jnp.concatenate(lat_list, axis=0)
    grad_key_rotary = jnp.concatenate(key_rot_list, axis=0)
    mixed_low = lax.optimization_barrier(mixed.astype(jnp.bfloat16)).astype(wide)
    grad_query_main = (factor * jnp.einsum("thl,lhd->thd", mixed_low, key_proj)).reshape(count, HEADS * KDIM)
    grad_query_rotary = (factor * rot_sum).reshape(count, HEADS * RDIM)
    grad_key_weight = (factor * jnp.einsum("thl,thd->lhd", mixed_low, main_query)).reshape(LATENT, HEADS * KDIM)
    return (grad_query_main, grad_query_rotary, grad_latent, grad_key_rotary, grad_key_weight)
```

```python
import functools
import math

import jax
import jax.numpy as jnp
from jax import lax
from jax.experimental import pallas as pl
from jax.experimental.pallas import tpu as pltpu
from jax.sharding import PartitionSpec as P

VMEM_BYTES = 67043328
MESH = pl.DeviceIdType.MESH
F32 = jnp.float32
BF16 = jnp.bfloat16
NX = 4
NY = 4
NZ = 16
SPAN = 4
TOK = 128
HEADS = 4
DIM = 128
RDIM = 64
WIDTH = 512
ROWS = 2 * HEADS * TOK
QUART = TOK // NY
WIDE = WIDTH + 128
PAIR = 2 * WIDTH + 128
STEPS = 2 * SPAN
SLOTS = 4
PART = 4
FACTOR = (DIM + RDIM) ** (-0.5)

DMA = pltpu.SemaphoreType.DMA


def dot(a, b, ca, cb, precision=None):
    return lax.dot_general(
        a, b, (((ca,), (cb,)), ((), ())), preferred_element_type=F32, precision=precision
    )


SCRATCH = dict(
    klat=pltpu.VMEM((SPAN, NX, TOK, WIDTH), BF16),
    krot=pltpu.VMEM((SPAN, NX, RDIM, TOK), BF16),
    qm=pltpu.VMEM((2, TOK, HEADS * DIM), BF16),
    og=pltpu.VMEM((2, TOK, HEADS * DIM), BF16),
    ho=pltpu.VMEM((2, TOK, HEADS * DIM), BF16),
    qr=pltpu.VMEM((2, TOK, HEADS * RDIM), BF16),
    lg=pltpu.VMEM((2, HEADS, TOK), F32),
    kw=pltpu.VMEM((WIDTH, HEADS * DIM), BF16),
    vw=pltpu.VMEM((WIDTH, HEADS * DIM), BF16),
    ql=pltpu.VMEM((ROWS, WIDTH), BF16),
    gr=pltpu.VMEM((ROWS, WIDTH), BF16),
    qrd=pltpu.VMEM((ROWS, 128), BF16),
    trow=pltpu.VMEM((1, ROWS), F32),
    lrow=pltpu.VMEM((1, ROWS), F32),
    mixed=pltpu.VMEM((ROWS, WIDTH), F32),
    rsum=pltpu.VMEM((ROWS, RDIM), F32),
    gf=pltpu.VMEM((SLOTS, NY, QUART, PAIR), F32),
    gst=pltpu.VMEM((STEPS, NY, QUART, PAIR), BF16),
    yin=pltpu.VMEM((STEPS, NY - 1, QUART, PAIR), BF16),
    xacc=pltpu.VMEM((SPAN, QUART, WIDE), F32),
    xst=pltpu.VMEM((SPAN, NX, QUART, WIDE), BF16),
    xin=pltpu.VMEM((SPAN, NX, QUART, WIDE), BF16),
    zst=pltpu.VMEM((SPAN, QUART, WIDE), BF16),
    zin=pltpu.VMEM((SPAN, QUART, WIDE), BF16),
    facc=pltpu.VMEM((QUART, WIDE), F32),
    obuf=pltpu.VMEM((NY, QUART, WIDE), F32),
    mrecv=pltpu.VMEM((ROWS, WIDTH // 2), F32),
    ml=pltpu.VMEM((ROWS, WIDTH // 2), BF16),
    rrecv=pltpu.VMEM((ROWS // 2, RDIM), F32),
    osend=pltpu.VMEM((TOK, HEADS * DIM), F32),
    orecv=pltpu.VMEM((TOK, HEADS * DIM), F32),
    kf=pltpu.VMEM((NX, 8, 8, HEADS * DIM), F32),
    kst=pltpu.VMEM((NX, 8, 8, HEADS * DIM), BF16),
    kxin=pltpu.VMEM((NX, 8, 8, HEADS * DIM), BF16),
    kz=pltpu.VMEM((8, 2, PART, HEADS * DIM), BF16),
    kzin=pltpu.VMEM((NZ, PART, HEADS * DIM), BF16),
    insem=DMA((9,)),
    qss=DMA((5,)), qrs=DMA((5,)),
    zks=DMA((SPAN, 2)), zkr=DMA((SPAN, 2)),
    xks=DMA((SPAN, NX, 2)), xkr=DMA((SPAN, NX, 2)),
    yss=DMA((STEPS, NY - 1)), yrs=DMA((STEPS, NY - 1)),
    xss=DMA((SPAN, NX)), xrs=DMA((SPAN, NX)),
    zss=DMA((SPAN,)), zrs=DMA((SPAN,)),
    mss=DMA((3,)), mrs=DMA((3,)),
    kxs=DMA((NX,)), kxr=DMA((NX,)),
    kzs=DMA((8, 2)), kzr=DMA((NZ,)),
    ags=DMA((NY - 1,)), agr=DMA((NY - 1,)),
)
NAMES = tuple(SCRATCH)


def rdma(src, dst, ss, rs, dev):
    return pltpu.make_async_remote_copy(
        src_ref=src, dst_ref=dst, send_sem=ss, recv_sem=rs, device_id=dev, device_id_type=MESH
    )


def kernel(qm_h, qr_h, lat_h, rot_h, kw_h, vw_h, ho_h, og_h, lg_h,
           o_main, o_rot, o_lat, o_krot, o_kw, *scratch):
    v = dict(zip(NAMES, scratch))
    klat, krot, ql, gr, qrd = v["klat"], v["krot"], v["ql"], v["gr"], v["qrd"]
    mixed, rsum, gf, gst, yin = v["mixed"], v["rsum"], v["gf"], v["gst"], v["yin"]
    trow, lrow = v["trow"], v["lrow"]
    sp = lax.axis_index("sp")
    tp = lax.axis_index("tp")
    z = sp // (2 * NX)
    x = (sp // 2) % NX
    c = sp % 2
    other = 1 - c
    xh = x // 2
    seq = (z + 1) // SPAN
    zz = z - jnp.maximum(seq * SPAN - 1, 0)
    after = jnp.minimum(seq * SPAN + SPAN - 1, NZ) - 1 - z
    partner = {"sp": sp + 1 - 2 * c}

    def at_x(xp):
        return {"sp": sp + 2 * (xp - x)}

    def at_y(yp):
        return {"tp": yp}

    barrier = pltpu.get_barrier_semaphore()

    @pl.loop(1, NZ)
    def _(d):
        zp = (z + d) % NZ
        for cp in range(2):
            pl.semaphore_signal(
                barrier, inc=1, device_id={"sp": zp * 2 * NX + 2 * x + cp}, device_id_type=MESH
            )

    pl.semaphore_signal(barrier, inc=1, device_id=partner, device_id_type=MESH)
    for d in range(1, NX):
        pl.semaphore_signal(barrier, inc=1, device_id=at_x((x + d) % NX), device_id_type=MESH)
    for d in range(1, NY):
        pl.semaphore_signal(barrier, inc=1, device_id=at_y((tp + d) % NY), device_id_type=MESH)

    shared = ("qm", "og", "ho", "qr", "lg")
    sources = (qm_h, og_h, ho_h, qr_h, lg_h)
    loads = [
        pltpu.make_async_copy(lat_h, klat.at[0, x], v["insem"].at[0]),
        pltpu.make_async_copy(rot_h, krot.at[0, x], v["insem"].at[1]),
    ]
    loads += [
        pltpu.make_async_copy(src, v[name].at[c], v["insem"].at[2 + n])
        for n, (name, src) in enumerate(zip(shared, sources))
    ]
    loads += [
        pltpu.make_async_copy(kw_h, v["kw"], v["insem"].at[7]),
        pltpu.make_async_copy(vw_h, v["vw"], v["insem"].at[8]),
    ]
    for cp in loads:
        cp.start()
    mixed[...] = jnp.zeros_like(mixed)
    rsum[...] = jnp.zeros_like(rsum)
    for cp in loads:
        cp.wait()

    def prepare(b):
        for h in range(HEADS):
            start = pl.multiple_of(b * (HEADS * TOK) + h * TOK, TOK)
            rows = pl.ds(start, TOK)
            cols = slice(h * DIM, (h + 1) * DIM)
            ql[rows] = dot(v["qm"][b, :, cols], v["kw"][:, cols], 1, 1).astype(BF16)
            og = v["og"][b, :, cols]
            gr[rows] = dot(og, v["vw"][:, cols], 1, 1).astype(BF16)
            rot = v["qr"][b, :, h * RDIM : (h + 1) * RDIM]
            qrd[rows] = jnp.concatenate([rot, rot], axis=1)
            prod = v["ho"][b, :, cols].astype(F32) * og.astype(F32)
            trow[:, rows] = dot(jnp.ones((8, DIM), F32), prod, 1, 1, lax.Precision.HIGHEST)[0:1]
            lrow[:, rows] = v["lg"][b, h : h + 1, :]

    def share(n, name):
        return rdma(v[name].at[c], v[name].at[c], v["qss"].at[n], v["qrs"].at[n], partner)

    def share_in(n, name):
        return rdma(v[name].at[other], v[name].at[other], v["qss"].at[n], v["qrs"].at[n], partner)

    keys = (klat, krot)

    def z_keys(d):
        return [
            rdma(k.at[0, x], k.at[d, x], v["zks"].at[d, n], v["zkr"].at[d, n], {"sp": sp + 2 * NX * d})
            for n, k in enumerate(keys)
        ]

    def x_keys(g, xp):
        return [
            rdma(k.at[g, x], k.at[g, x], v["xks"].at[g, xp, n], v["xkr"].at[g, x, n], at_x(xp))
            for n, k in enumerate(keys)
        ]

    def x_keys_in(g, xp):
        return [
            rdma(k.at[g, xp], k.at[g, xp], v["xks"].at[g, xp, n], v["xkr"].at[g, xp, n], at_x(xp))
            for n, k in enumerate(keys)
        ]

    prepare(c)
    pl.semaphore_wait(barrier, 2 * (NZ - 1) + 1 + NX - 1 + NY - 1)

    for n, name in enumerate(shared):
        share(n, name).start()
    for d in (1, 3, 2):
        xp = (x + d) % NX

        @pl.when(xp >= 2 * xh)
        def _():
            for cp in x_keys(0, xp):
                cp.start()

    @pl.loop(1, after + 1)
    def _(d):
        for cp in z_keys(d):
            cp.start()

    for n, name in enumerate(shared):
        share_in(n, name).wait_recv()
    prepare(other)

    def forward(g):
        @pl.when(g <= zz)
        def _():
            for cp in z_keys(g):
                cp.wait_recv()
            for d in (1, 3, 2):
                for cp in x_keys(g, (x + d) % NX):
                    cp.start()

    forward(1)

    first = 1 - xh
    last = 2 * zz + 1

    def y_copy(s, d):
        return rdma(
            gst.at[s, (tp + d) % NY], yin.at[s, d - 1], v["yss"].at[s, d - 1], v["yrs"].at[s, d - 1],
            at_y((tp + d) % NY),
        )

    def attend(s):
        g = s // 2
        m = 1 - s % 2
        for b in range(2):
            xp = 2 * m + b

            @pl.when(xp != x)
            def _():
                for cp in x_keys_in(g, xp):
                    cp.wait_recv()

        lt = klat[g, pl.ds(2 * m, 2)].reshape(2 * TOK, WIDTH)
        rt = jnp.concatenate([krot[g, 2 * m], krot[g, 2 * m + 1]], axis=1)
        scores = dot(lt, ql[...], 1, 1) + dot(rt, qrd[:, :RDIM], 0, 1)
        weights = jnp.exp(FACTOR * scores - lrow[...])
        k_id = lax.broadcasted_iota(jnp.int32, (2 * TOK, 1), 0)
        k_pos = (2 * m + k_id // TOK) * (2 * TOK) + c * TOK + k_id % TOK
        k_pos = jnp.where(g > 0, -1, k_pos)
        q_id = lax.broadcasted_iota(jnp.int32, (1, ROWS), 1)
        q_pos = (2 * x + q_id // (HEADS * TOK)) * TOK + q_id % TOK
        weights = jnp.where(k_pos <= q_pos, weights, 0.0)
        slopes = dot(lt, gr[...], 1, 1)
        dscores = weights * (slopes - trow[...])
        wl = weights.astype(BF16)
        dl = dscores.astype(BF16)
        grad = FACTOR * dot(dl, ql[...], 1, 0) + dot(wl, gr[...], 1, 0)
        slot = s % SLOTS
        gf[slot, :, :, :WIDTH] = grad[:TOK].reshape(NY, QUART, WIDTH)
        gf[slot, :, :, WIDTH : 2 * WIDTH] = grad[TOK:].reshape(NY, QUART, WIDTH)
        rgrad = FACTOR * dot(dl, qrd[...], 1, 0)
        lane = lax.broadcasted_iota(jnp.int32, (TOK, 128), 1)
        packed = jnp.where(lane < RDIM, rgrad[:TOK], rgrad[TOK:])
        gf[slot, :, :, 2 * WIDTH :] = packed.reshape(NY, QUART, 128)
        gst[s] = gf[slot].astype(BF16)
        for d in (1, 3, 2):
            y_copy(s, d).start()
        mixed[...] += dot(dl, lt, 0, 0)
        rsum[...] += dot(dl, rt, 0, 1)

    def x_copy(g, xp):
        return rdma(
            v["xst"].at[g, xp], v["xin"].at[g, x], v["xss"].at[g, xp], v["xrs"].at[g, x], at_x(xp)
        )

    def x_copy_in(g, xp):
        return rdma(
            v["xst"].at[g, xp], v["xin"].at[g, xp], v["xss"].at[g, xp], v["xrs"].at[g, xp], at_x(xp)
        )

    def reduce_y(s):
        @pl.when((s >= first) & (s <= last))
        def _():
            g = s // 2
            m = 1 - s % 2
            total = gf[s % SLOTS, tp]
            for d in range(1, NY):
                y_copy(s, d).wait_recv()
                total = total + yin[s, d - 1].astype(F32)
            for b in range(2):
                xp = 2 * m + b
                lat = total[:, b * WIDTH : (b + 1) * WIDTH]
                rot = total[:, 2 * WIDTH :]

                @pl.when(xp == x)
                def _():
                    v["xacc"][g, :, :WIDTH] = lat
                    v["xacc"][g, :, WIDTH:] = rot

                @pl.when(xp != x)
                def _():
                    v["xst"][g, xp, :, :WIDTH] = lat.astype(BF16)
                    v["xst"][g, xp, :, WIDTH:] = rot.astype(BF16)
                    x_copy(g, xp).start()

    def z_copy(g):
        return rdma(
            v["zst"].at[g], v["zin"].at[g], v["zss"].at[g], v["zrs"].at[g], {"sp": sp - 2 * NX * g}
        )

    def reduce_x(s):
        @pl.when((s >= first) & (s <= last) & (s % 2 == first))
        def _():
            g = s // 2
            v["facc"][...] = v["xacc"][g]
            for d in range(1, NX):
                xp = (x + d) % NX

                @pl.when((g > 0) | (xp >= 2 * xh))
                def _():
                    x_copy_in(g, xp).wait_recv()
                    v["facc"][...] += v["xin"][g, xp].astype(F32)

            @pl.when(g > 0)
            def _():
                v["zst"][g] = v["facc"][...].astype(BF16)
                z_copy(g).start()

            @pl.when(g == 0)
            def _():
                v["obuf"][tp] = v["facc"][...]

    @pl.loop(first, last + 1)
    def _(s):
        attend(s)

        @pl.when(s % 2 == 1)
        def _():
            forward((s + 3) // 2)

        reduce_y(s - 2)
        reduce_x(s - 3)

    half = WIDTH // 2
    mine = pl.ds(pl.multiple_of(half * c, half), half)
    theirs = pl.ds(pl.multiple_of(half * other, half), half)
    my_rows = pl.ds(pl.multiple_of(c * (ROWS // 2), ROWS // 2), ROWS // 2)
    their_rows = pl.ds(pl.multiple_of(other * (ROWS // 2), ROWS // 2), ROWS // 2)
    mix_copy = rdma(mixed.at[:, theirs], v["mrecv"], v["mss"].at[0], v["mrs"].at[0], partner)
    rot_copy = rdma(rsum.at[their_rows], v["rrecv"], v["mss"].at[1], v["mrs"].at[1], partner)
    main_copy = rdma(v["osend"], v["orecv"], v["mss"].at[2], v["mrs"].at[2], partner)
    mix_copy.start()
    rot_copy.start()
    reduce_y(last - 1)
    reduce_x(last - 2)

    mix_copy.wait_recv()
    ml = v["ml"]
    ml[...] = (mixed[:, mine] + v["mrecv"][...]).astype(BF16)

    def main_part(b, h):
        rows = pl.ds(pl.multiple_of(b * (HEADS * TOK) + h * TOK, TOK), TOK)
        return dot(ml[rows], v["kw"][mine, h * DIM : (h + 1) * DIM], 1, 0)

    for h in range(HEADS):
        v["osend"][:, h * DIM : (h + 1) * DIM] = main_part(other, h)
    main_copy.start()
    for h in range(HEADS):
        cols = slice(h * DIM, (h + 1) * DIM)
        left = jnp.concatenate(
            [ml[b * HEADS * TOK + h * TOK : b * HEADS * TOK + (h + 1) * TOK] for b in range(2)], axis=0
        )
        right = jnp.concatenate([v["qm"][b, :, cols] for b in range(2)], axis=0)
        term = (FACTOR * dot(left, right, 0, 0)).reshape(8, NX, 8, DIM)
        for xp in range(NX):
            v["kf"][xp, :, :, cols] = term[:, xp]
            v["kst"][xp, :, :, cols] = term[:, xp].astype(BF16)

    def kx_copy(xp):
        return rdma(v["kst"].at[xp], v["kxin"].at[x], v["kxs"].at[xp], v["kxr"].at[x], at_x(xp))

    def kx_copy_in(xp):
        return rdma(v["kst"].at[xp], v["kxin"].at[xp], v["kxs"].at[xp], v["kxr"].at[xp], at_x(xp))

    for d in (1, 3, 2):
        kx_copy((x + d) % NX).start()

    reduce_y(last)
    reduce_x(last - 1)
    reduce_x(last)

    total = v["kf"][x]
    for d in range(1, NX):
        xp = (x + d) % NX
        kx_copy_in(xp).wait_recv()
        total = total + v["kxin"][xp].astype(F32)
    total = total.astype(BF16)
    v["kz"][:, 0] = total[:, :PART]
    v["kz"][:, 1] = total[:, PART:]

    def kz_copy(zp, cp):
        return rdma(
            v["kz"].at[zp, cp], v["kzin"].at[z], v["kzs"].at[zp, cp], v["kzr"].at[z],
            {"sp": (8 * c + zp) * 2 * NX + 2 * x + cp},
        )

    @pl.loop(0, 8)
    def _(i):
        zp = (z + i) % 8
        for cp in range(2):
            here = (8 * c + zp == z) & (c == cp)

            @pl.when(jnp.logical_not(here))
            def _():
                kz_copy(zp, cp).start()

            @pl.when(here)
            def _():
                v["kzin"][z] = v["kz"][zp, cp]

    rot_copy.wait_recv()
    for h in range(HEADS):
        rows = pl.ds(pl.multiple_of(c * (HEADS * TOK) + h * TOK, TOK), TOK)
        o_rot[:, h * RDIM : (h + 1) * RDIM] = FACTOR * (
            rsum[rows] + v["rrecv"][h * TOK : (h + 1) * TOK]
        )
    main_copy.wait_recv()
    for h in range(HEADS):
        cols = slice(h * DIM, (h + 1) * DIM)
        o_main[:, cols] = FACTOR * (main_part(c, h) + v["orecv"][:, cols])

    @pl.loop(1, after + 1)
    def _(d):
        z_copy_in = rdma(
            v["zst"].at[d], v["zin"].at[d], v["zss"].at[d], v["zrs"].at[d], {"sp": sp + 2 * NX * d}
        )
        z_copy_in.wait_recv()
        v["obuf"][tp] += v["zin"][d].astype(F32)

    def ag_copy(d):
        return rdma(
            v["obuf"].at[tp], v["obuf"].at[tp], v["ags"].at[d - 1], v["agr"].at[d - 1],
            at_y((tp + d) % NY),
        )

    for d in (1, 3, 2):
        ag_copy(d).start()

    @pl.loop(0, NZ)
    def _(i):
        @pl.when((i != z) | (c != z // 8))
        def _():
            rdma(
                v["kz"].at[0, 0], v["kzin"].at[i], v["kzs"].at[0, 0], v["kzr"].at[i],
                {"sp": i * 2 * NX + 2 * x + z // 8},
            ).wait_recv()

    total = v["kzin"][0].astype(F32)
    for i in range(1, NZ):
        total = total + v["kzin"][i].astype(F32)
    o_kw[...] = total

    for d in range(1, NY):
        yp = (tp + NY - d) % NY
        rdma(
            v["obuf"].at[yp], v["obuf"].at[yp], v["ags"].at[d - 1], v["agr"].at[d - 1], at_y(yp)
        ).wait_recv()
    out = v["obuf"][...].reshape(TOK, WIDE)
    o_lat[...] = out[:, :WIDTH]
    flip = out[:, WIDTH:].T
    o_krot[...] = jnp.where(x % 2 == 0, flip[:RDIM], flip[RDIM:])

    for n, name in enumerate(shared):
        share(n, name).wait_send()
    for d in range(1, NX):
        xp = (x + d) % NX

        @pl.when(xp >= 2 * xh)
        def _():
            for cp in x_keys(0, xp):
                cp.wait_send()

        kx_copy(xp).wait_send()

        @pl.loop(1, zz + 1)
        def _(g):
            for cp in x_keys(g, xp):
                cp.wait_send()

        @pl.loop(0, zz + 1)
        def _(g):
            @pl.when((g > 0) | (xp // 2 <= xh))
            def _():
                x_copy(g, xp).wait_send()

    @pl.loop(1, after + 1)
    def _(d):
        for cp in z_keys(d):
            cp.wait_send()

    @pl.loop(1, zz + 1)
    def _(g):
        z_copy(g).wait_send()

    @pl.loop(first, last + 1)
    def _(s):
        for d in range(1, NY):
            y_copy(s, d).wait_send()

    mix_copy.wait_send()
    rot_copy.wait_send()
    main_copy.wait_send()

    @pl.loop(0, 8)
    def _(zp):
        for cp in range(2):
            @pl.when((8 * c + zp != z) | (c != cp))
            def _():
                kz_copy(zp, cp).wait_send()

    for d in range(1, NY):
        ag_copy(d).wait_send()


def store(*refs):
    *pairs, sem = refs
    count = len(pairs) // 2
    copies = [
        pltpu.make_async_copy(pairs[n], pairs[count + n], sem.at[n]) for n in range(count)
    ]
    for cp in copies:
        cp.start()
    for cp in copies:
        cp.wait()


def per_device(qm, qr, lat, rot, kw, vw, ho, og, logs):
    args = (qm, qr, lat, rot.T, kw, vw, ho, og, logs)
    shapes = (
        (TOK, HEADS * DIM), (TOK, HEADS * RDIM), (TOK, WIDTH), (RDIM, TOK), (PART, HEADS * DIM),
    )
    results = sum(4 * math.prod(s) for s in shapes)
    vmem = pl.BlockSpec(memory_space=pltpu.VMEM)
    hbm = pl.BlockSpec(memory_space=pltpu.HBM)
    held = pl.pallas_call(
        kernel,
        out_shape=[pltpu.VMEM(s, F32) for s in shapes],
        in_specs=[hbm] * len(args),
        out_specs=[vmem] * len(shapes),
        scratch_shapes=list(SCRATCH.values()),
        compiler_params=pltpu.CompilerParams(
            collective_id=0, has_side_effects=True, vmem_limit_bytes=VMEM_BYTES - results - (16 << 10)
        ),
        name="latent_attention_backward",
    )(*args)
    main, rotary, lat_out, rot_out, weight = pl.pallas_call(
        store,
        out_shape=[jax.ShapeDtypeStruct(s, F32) for s in shapes],
        in_specs=[vmem] * len(shapes),
        out_specs=[hbm] * len(shapes),
        scratch_shapes=[DMA((len(shapes),))],
        compiler_params=pltpu.CompilerParams(vmem_limit_bytes=4 << 20),
        name="store_outputs",
    )(*held)
    return main, rotary, lat_out, rot_out.T, weight


def solution(mesh):
    return jax.shard_map(
        per_device,
        mesh=mesh,
        in_specs=(
            P("sp", "tp"),
            P("sp", "tp"),
            P("sp", None),
            P("sp", None),
            P(None, "tp"),
            P(None, "tp"),
            P("sp", "tp"),
            P("sp", "tp"),
            P("tp", "sp"),
        ),
        out_specs=(P("sp", "tp"), P("sp", "tp"), P("sp", None), P("sp", None), P("sp", "tp")),
        check_vma=False,
    )
```

```python
import functools
import math

import jax
import jax.numpy as jnp
from jax import lax
from jax.experimental import pallas as pl
from jax.experimental.pallas import tpu as pltpu
from jax.sharding import PartitionSpec as P

VMEM_BYTES = 67043328
MESH = pl.DeviceIdType.MESH
F32 = jnp.float32
BF16 = jnp.bfloat16
NX = 4
NY = 4
NZ = 16
SPAN = 4
TOK = 128
HEADS = 4
DIM = 128
RDIM = 64
WIDTH = 512
ROWS = 2 * HEADS * TOK
QUART = TOK // NY
WIDE = WIDTH + 128
PAIR = 2 * WIDTH + 128
STEPS = 2 * SPAN
SLOTS = 4
PART = 4
FACTOR = (DIM + RDIM) ** (-0.5)

DMA = pltpu.SemaphoreType.DMA


def dot(a, b, ca, cb, precision=None):
    return lax.dot_general(
        a, b, (((ca,), (cb,)), ((), ())), preferred_element_type=F32, precision=precision
    )


SCRATCH = dict(
    klat=pltpu.VMEM((SPAN, NX, TOK, WIDTH), BF16),
    krot=pltpu.VMEM((SPAN, NX, RDIM, TOK), BF16),
    qm=pltpu.VMEM((2, TOK, HEADS * DIM), BF16),
    og=pltpu.VMEM((2, TOK, HEADS * DIM), BF16),
    ho=pltpu.VMEM((2, TOK, HEADS * DIM), BF16),
    qr=pltpu.VMEM((2, TOK, HEADS * RDIM), BF16),
    lg=pltpu.VMEM((2, HEADS, TOK), F32),
    kw=pltpu.VMEM((WIDTH, HEADS * DIM), BF16),
    vw=pltpu.VMEM((WIDTH, HEADS * DIM), BF16),
    ql=pltpu.VMEM((ROWS, WIDTH), BF16),
    gr=pltpu.VMEM((ROWS, WIDTH), BF16),
    qrd=pltpu.VMEM((ROWS, 128), BF16),
    trow=pltpu.VMEM((1, ROWS), F32),
    lrow=pltpu.VMEM((1, ROWS), F32),
    mixed=pltpu.VMEM((ROWS, WIDTH), F32),
    rsum=pltpu.VMEM((ROWS, RDIM), F32),
    gf=pltpu.VMEM((SLOTS, NY, QUART, PAIR), F32),
    gst=pltpu.VMEM((STEPS, NY, QUART, PAIR), BF16),
    yin=pltpu.VMEM((STEPS, NY - 1, QUART, PAIR), BF16),
    xacc=pltpu.VMEM((SPAN, QUART, WIDE), F32),
    xst=pltpu.VMEM((SPAN, NX, QUART, WIDE), BF16),
    xin=pltpu.VMEM((SPAN, NX, QUART, WIDE), BF16),
    zst=pltpu.VMEM((SPAN, QUART, WIDE), BF16),
    zin=pltpu.VMEM((SPAN, QUART, WIDE), BF16),
    facc=pltpu.VMEM((QUART, WIDE), F32),
    obuf=pltpu.VMEM((NY, QUART, WIDE), F32),
    mrecv=pltpu.VMEM((ROWS, WIDTH // 2), F32),
    ml=pltpu.VMEM((ROWS, WIDTH // 2), BF16),
    rrecv=pltpu.VMEM((ROWS // 2, RDIM), F32),
    osend=pltpu.VMEM((TOK, HEADS * DIM), F32),
    orecv=pltpu.VMEM((TOK, HEADS * DIM), F32),
    kf=pltpu.VMEM((NX, 8, 8, HEADS * DIM), F32),
    kst=pltpu.VMEM((NX, 8, 8, HEADS * DIM), BF16),
    kxin=pltpu.VMEM((NX, 8, 8, HEADS * DIM), BF16),
    kz=pltpu.VMEM((8, 2, PART, HEADS * DIM), BF16),
    kzin=pltpu.VMEM((NZ, PART, HEADS * DIM), BF16),
    insem=DMA((9,)),
    qss=DMA((5,)), qrs=DMA((5,)),
    zks=DMA((SPAN, 2)), zkr=DMA((SPAN, 2)),
    xks=DMA((SPAN, NX, 2)), xkr=DMA((SPAN, NX, 2)),
    yss=DMA((STEPS, NY - 1)), yrs=DMA((STEPS, NY - 1)),
    fks=DMA((SPAN, 2, 2)), fkr=DMA((SPAN, 2, 2)),
    far=pltpu.SemaphoreType.REGULAR((3,)),
    xss=DMA((SPAN, NX)), xrs=DMA((SPAN, NX)),
    zss=DMA((SPAN,)), zrs=DMA((SPAN,)),
    mss=DMA((3,)), mrs=DMA((3,)),
    kxs=DMA((NX,)), kxr=DMA((NX,)),
    kzs=DMA((8, 2)), kzr=DMA((NZ,)),
    ags=DMA((NY - 1,)), agr=DMA((NY - 1,)),
)
NAMES = tuple(SCRATCH)


def rdma(src, dst, ss, rs, dev):
    return pltpu.make_async_remote_copy(
        src_ref=src, dst_ref=dst, send_sem=ss, recv_sem=rs, device_id=dev, device_id_type=MESH
    )


def kernel(qm_h, qr_h, lat_h, rot_h, kw_h, vw_h, ho_h, og_h, lg_h,
           o_main, o_rot, o_lat, o_krot, o_kw, *scratch):
    v = dict(zip(NAMES, scratch))
    klat, krot, ql, gr, qrd = v["klat"], v["krot"], v["ql"], v["gr"], v["qrd"]
    mixed, rsum, gf, gst, yin = v["mixed"], v["rsum"], v["gf"], v["gst"], v["yin"]
    trow, lrow = v["trow"], v["lrow"]
    sp = lax.axis_index("sp")
    tp = lax.axis_index("tp")
    z = sp // (2 * NX)
    x = (sp // 2) % NX
    c = sp % 2
    other = 1 - c
    xh = x // 2
    near = x + 1 - 2 * (x % 2)
    far = (x + 2) % NX
    side = NX - 1 - x
    seq = (z + 1) // SPAN
    zz = z - jnp.maximum(seq * SPAN - 1, 0)
    after = jnp.minimum(seq * SPAN + SPAN - 1, NZ) - 1 - z
    partner = {"sp": sp + 1 - 2 * c}

    def at_x(xp):
        return {"sp": sp + 2 * (xp - x)}

    def at_y(yp):
        return {"tp": yp}

    barrier = pltpu.get_barrier_semaphore()

    def at_z(d, cp):
        return {"sp": ((z + NZ + d) % NZ) * 2 * NX + 2 * x + cp}

    for d in (1, -1):
        for cp in range(2):
            pl.semaphore_signal(barrier, inc=1, device_id=at_z(d, cp), device_id_type=MESH)
    pl.semaphore_signal(barrier, inc=1, device_id=partner, device_id_type=MESH)
    for d in range(1, NX):
        pl.semaphore_signal(barrier, inc=1, device_id=at_x((x + d) % NX), device_id_type=MESH)
    for d in range(1, NY):
        pl.semaphore_signal(barrier, inc=1, device_id=at_y((tp + d) % NY), device_id_type=MESH)

    shared = ("qm", "og", "ho", "qr", "lg")
    sources = (qm_h, og_h, ho_h, qr_h, lg_h)
    loads = [
        pltpu.make_async_copy(lat_h, klat.at[0, x], v["insem"].at[0]),
        pltpu.make_async_copy(rot_h, krot.at[0, x], v["insem"].at[1]),
    ]
    loads += [
        pltpu.make_async_copy(src, v[name].at[c], v["insem"].at[2 + n])
        for n, (name, src) in enumerate(zip(shared, sources))
    ]
    loads += [
        pltpu.make_async_copy(kw_h, v["kw"], v["insem"].at[7]),
        pltpu.make_async_copy(vw_h, v["vw"], v["insem"].at[8]),
    ]
    for cp in loads:
        cp.start()
    mixed[...] = jnp.zeros_like(mixed)
    rsum[...] = jnp.zeros_like(rsum)
    for cp in loads:
        cp.wait()

    def prepare(b):
        for h in range(HEADS):
            start = pl.multiple_of(b * (HEADS * TOK) + h * TOK, TOK)
            rows = pl.ds(start, TOK)
            cols = slice(h * DIM, (h + 1) * DIM)
            ql[rows] = dot(v["qm"][b, :, cols], v["kw"][:, cols], 1, 1).astype(BF16)
            og = v["og"][b, :, cols]
            gr[rows] = dot(og, v["vw"][:, cols], 1, 1).astype(BF16)
            rot = v["qr"][b, :, h * RDIM : (h + 1) * RDIM]
            qrd[rows] = jnp.concatenate([rot, rot], axis=1)
            prod = v["ho"][b, :, cols].astype(F32) * og.astype(F32)
            trow[:, rows] = dot(jnp.ones((8, DIM), F32), prod, 1, 1, lax.Precision.HIGHEST)[0:1]
            lrow[:, rows] = v["lg"][b, h : h + 1, :]

    def share(n, name):
        return rdma(v[name].at[c], v[name].at[c], v["qss"].at[n], v["qrs"].at[n], partner)

    def share_in(n, name):
        return rdma(v[name].at[other], v[name].at[other], v["qss"].at[n], v["qrs"].at[n], partner)

    keys = (klat, krot)

    def z_keys(d):
        return [
            rdma(k.at[0, x], k.at[d, x], v["zks"].at[d, n], v["zkr"].at[d, n], {"sp": sp + 2 * NX * d})
            for n, k in enumerate(keys)
        ]

    def x_keys(g, xp):
        return [
            rdma(k.at[g, x], k.at[g, x], v["xks"].at[g, xp, n], v["xkr"].at[g, x, n], at_x(xp))
            for n, k in enumerate(keys)
        ]

    def x_keys_in(g, xp):
        return [
            rdma(k.at[g, xp], k.at[g, xp], v["xks"].at[g, xp, n], v["xkr"].at[g, xp, n], at_x(xp))
            for n, k in enumerate(keys)
        ]

    prepare(c)
    pl.semaphore_wait(barrier, 4 + 1 + NX - 1 + NY - 1)

    def greet(n):
        for d in (1, -1):
            pl.semaphore_signal(
                v["far"].at[n], inc=1, device_id=at_z(d << n, c), device_id_type=MESH
            )

    def met(n):
        pl.semaphore_wait(v["far"].at[n], 2)

    greet(0)

    for n, name in enumerate(shared):
        share(n, name).start()

    def send_up(d):
        @pl.when(d <= after)
        def _():
            for cp in z_keys(d):
                cp.start()

    send_up(1)
    for xp in (near, side, far):
        @pl.when(xp >= 2 * xh)
        def _():
            for cp in x_keys(0, xp):
                cp.start()

    for n, name in enumerate(shared):
        share_in(n, name).wait_recv()
    prepare(other)
    met(0)
    send_up(2)
    greet(1)

    def forward(g):
        @pl.when(g <= zz)
        def _():
            for cp in z_keys(g):
                cp.wait_recv()
            for xp in (near, side):
                for cp in x_keys(g, xp):
                    cp.start()

    forward(1)
    last = 2 * zz + 1

    def pass_on(g, i):
        src, dst = ((near, side), (side, near))[i]
        out = []
        for n, (k, size) in enumerate(((klat, TOK // 2), (krot, RDIM // 2))):
            part = k.at[g, src, pl.ds(i * size, size)]
            out.append(
                rdma(part, part, v["fks"].at[g, i, n], v["fkr"].at[g, i, n], at_x(dst))
            )
        return out

    def passed_in(g, i):
        out = []
        for n, (k, size) in enumerate(((klat, TOK // 2), (krot, RDIM // 2))):
            part = k.at[g, far, pl.ds(i * size, size)]
            out.append(
                rdma(part, part, v["fks"].at[g, i, n], v["fkr"].at[g, i, n], at_x((near, side)[1 - i]))
            )
        return out

    def pair_of(s):
        return xh + (s % 2) * (1 - 2 * xh)

    def valid(s):
        return (s >= 0) & (s <= last) & ((s != 1) | (xh == 1))

    def y_copy(s, d):
        return rdma(
            gst.at[s, (tp + d) % NY], yin.at[s, d - 1], v["yss"].at[s, d - 1], v["yrs"].at[s, d - 1],
            at_y((tp + d) % NY),
        )

    def attend(s):
        g = s // 2
        m = pair_of(s)

        @pl.when(s % 2 == 0)
        def _():
            for cp in x_keys_in(g, near):
                cp.wait_recv()

            @pl.when(g > 0)
            def _():
                for cp in x_keys_in(g, side):
                    cp.wait_recv()
                for i in range(2):
                    for cp in pass_on(g, i):
                        cp.start()

        @pl.when((s % 2 == 1) & (g > 0))
        def _():
            for i in range(2):
                for cp in passed_in(g, i):
                    cp.wait_recv()

        @pl.when(s == 1)
        def _():
            for xp in (side, far):
                for cp in x_keys_in(0, xp):
                    cp.wait_recv()

        lt = klat[g, pl.ds(2 * m, 2)].reshape(2 * TOK, WIDTH)
        rt = jnp.concatenate([krot[g, 2 * m], krot[g, 2 * m + 1]], axis=1)
        scores = dot(lt, ql[...], 1, 1) + dot(rt, qrd[:, :RDIM], 0, 1)
        weights = jnp.exp(FACTOR * scores - lrow[...])
        k_id = lax.broadcasted_iota(jnp.int32, (2 * TOK, 1), 0)
        k_pos = (2 * m + k_id // TOK) * (2 * TOK) + c * TOK + k_id % TOK
        k_pos = jnp.where(g > 0, -1, k_pos)
        q_id = lax.broadcasted_iota(jnp.int32, (1, ROWS), 1)
        q_pos = (2 * x + q_id // (HEADS * TOK)) * TOK + q_id % TOK
        weights = jnp.where(k_pos <= q_pos, weights, 0.0)
        slopes = dot(lt, gr[...], 1, 1)
        dscores = weights * (slopes - trow[...])
        wl = weights.astype(BF16)
        dl = dscores.astype(BF16)
        grad = FACTOR * dot(dl, ql[...], 1, 0) + dot(wl, gr[...], 1, 0)
        slot = s % SLOTS
        gf[slot, :, :, :WIDTH] = grad[:TOK].reshape(NY, QUART, WIDTH)
        gf[slot, :, :, WIDTH : 2 * WIDTH] = grad[TOK:].reshape(NY, QUART, WIDTH)
        rgrad = FACTOR * dot(dl, qrd[...], 1, 0)
        lane = lax.broadcasted_iota(jnp.int32, (TOK, 128), 1)
        packed = jnp.where(lane < RDIM, rgrad[:TOK], rgrad[TOK:])
        gf[slot, :, :, 2 * WIDTH :] = packed.reshape(NY, QUART, 128)
        gst[s] = gf[slot].astype(BF16)
        for d in (1, 3, 2):
            y_copy(s, d).start()
        mixed[...] += dot(dl, lt, 0, 0)
        rsum[...] += dot(dl, rt, 0, 1)

    def x_copy(g, xp):
        return rdma(
            v["xst"].at[g, xp], v["xin"].at[g, x], v["xss"].at[g, xp], v["xrs"].at[g, x], at_x(xp)
        )

    def x_copy_in(g, xp):
        return rdma(
            v["xst"].at[g, xp], v["xin"].at[g, xp], v["xss"].at[g, xp], v["xrs"].at[g, xp], at_x(xp)
        )

    def reduce_y(s):
        @pl.when(valid(s))
        def _():
            g = s // 2
            m = pair_of(s)
            total = gf[s % SLOTS, tp]
            for d in range(1, NY):
                y_copy(s, d).wait_recv()
                total = total + yin[s, d - 1].astype(F32)
            for b in range(2):
                xp = 2 * m + b
                lat = total[:, b * WIDTH : (b + 1) * WIDTH]
                rot = total[:, 2 * WIDTH :]

                @pl.when(xp == x)
                def _():
                    v["xacc"][g, :, :WIDTH] = lat
                    v["xacc"][g, :, WIDTH:] = rot

                @pl.when(xp != x)
                def _():
                    v["xst"][g, xp, :, :WIDTH] = lat.astype(BF16)
                    v["xst"][g, xp, :, WIDTH:] = rot.astype(BF16)
                    x_copy(g, xp).start()

    def z_copy(g):
        return rdma(
            v["zst"].at[g], v["zin"].at[g], v["zss"].at[g], v["zrs"].at[g], {"sp": sp - 2 * NX * g}
        )

    def reduce_x(s):
        @pl.when((s >= 0) & (s <= last) & (s % 2 == 1))
        def _():
            g = s // 2
            v["facc"][...] = v["xacc"][g]
            for d in range(1, NX):
                xp = (x + d) % NX

                @pl.when((g > 0) | (xp >= 2 * xh))
                def _():
                    x_copy_in(g, xp).wait_recv()
                    v["facc"][...] += v["xin"][g, xp].astype(F32)

            @pl.when(g > 0)
            def _():
                v["zst"][g] = v["facc"][...].astype(BF16)
                z_copy(g).start()

            @pl.when(g == 0)
            def _():
                v["obuf"][tp] = v["facc"][...]

    @pl.loop(0, last + 1)
    def _(s):
        @pl.when(valid(s))
        def _():
            attend(s)

        @pl.when((s % 2 == 0) & (s > 0))
        def _():
            forward(s // 2 + 1)

        @pl.when(s == 0)
        def _():
            met(1)
            send_up(3)
            greet(2)

        reduce_y(s - 2)
        reduce_x(s - 3)

    half = WIDTH // 2
    mine = pl.ds(pl.multiple_of(half * c, half), half)
    theirs = pl.ds(pl.multiple_of(half * other, half), half)
    my_rows = pl.ds(pl.multiple_of(c * (ROWS // 2), ROWS // 2), ROWS // 2)
    their_rows = pl.ds(pl.multiple_of(other * (ROWS // 2), ROWS // 2), ROWS // 2)
    mix_copy = rdma(mixed.at[:, theirs], v["mrecv"], v["mss"].at[0], v["mrs"].at[0], partner)
    rot_copy = rdma(rsum.at[their_rows], v["rrecv"], v["mss"].at[1], v["mrs"].at[1], partner)
    main_copy = rdma(v["osend"], v["orecv"], v["mss"].at[2], v["mrs"].at[2], partner)
    mix_copy.start()
    rot_copy.start()
    reduce_y(last - 1)
    reduce_x(last - 2)

    mix_copy.wait_recv()
    ml = v["ml"]
    ml[...] = (mixed[:, mine] + v["mrecv"][...]).astype(BF16)

    def main_part(b, h):
        rows = pl.ds(pl.multiple_of(b * (HEADS * TOK) + h * TOK, TOK), TOK)
        return dot(ml[rows], v["kw"][mine, h * DIM : (h + 1) * DIM], 1, 0)

    for h in range(HEADS):
        v["osend"][:, h * DIM : (h + 1) * DIM] = main_part(other, h)
    main_copy.start()
    for h in range(HEADS):
        cols = slice(h * DIM, (h + 1) * DIM)
        left = jnp.concatenate(
            [ml[b * HEADS * TOK + h * TOK : b * HEADS * TOK + (h + 1) * TOK] for b in range(2)], axis=0
        )
        right = jnp.concatenate([v["qm"][b, :, cols] for b in range(2)], axis=0)
        term = (FACTOR * dot(left, right, 0, 0)).reshape(8, NX, 8, DIM)
        for xp in range(NX):
            v["kf"][xp, :, :, cols] = term[:, xp]
            v["kst"][xp, :, :, cols] = term[:, xp].astype(BF16)

    def kx_copy(xp):
        return rdma(v["kst"].at[xp], v["kxin"].at[x], v["kxs"].at[xp], v["kxr"].at[x], at_x(xp))

    def kx_copy_in(xp):
        return rdma(v["kst"].at[xp], v["kxin"].at[xp], v["kxs"].at[xp], v["kxr"].at[xp], at_x(xp))

    for d in (1, 3, 2):
        kx_copy((x + d) % NX).start()

    reduce_y(last)

    total = v["kf"][x]
    for d in range(1, NX):
        xp = (x + d) % NX
        kx_copy_in(xp).wait_recv()
        total = total + v["kxin"][xp].astype(F32)
    total = total.astype(BF16)
    v["kz"][:, 0] = total[:, :PART]
    v["kz"][:, 1] = total[:, PART:]

    def kz_copy(zp, cp):
        return rdma(
            v["kz"].at[zp, cp], v["kzin"].at[z], v["kzs"].at[zp, cp], v["kzr"].at[z],
            {"sp": (8 * c + zp) * 2 * NX + 2 * x + cp},
        )

    met(2)

    @pl.loop(0, 8)
    def _(i):
        zp = (z + i) % 8
        for cp in range(2):
            here = (8 * c + zp == z) & (c == cp)

            @pl.when(jnp.logical_not(here))
            def _():
                kz_copy(zp, cp).start()

            @pl.when(here)
            def _():
                v["kzin"][z] = v["kz"][zp, cp]

    reduce_x(last)
    rot_copy.wait_recv()
    for h in range(HEADS):
        rows = pl.ds(pl.multiple_of(c * (HEADS * TOK) + h * TOK, TOK), TOK)
        o_rot[:, h * RDIM : (h + 1) * RDIM] = FACTOR * (
            rsum[rows] + v["rrecv"][h * TOK : (h + 1) * TOK]
        )
    main_copy.wait_recv()
    for h in range(HEADS):
        cols = slice(h * DIM, (h + 1) * DIM)
        o_main[:, cols] = FACTOR * (main_part(c, h) + v["orecv"][:, cols])

    @pl.loop(1, after + 1)
    def _(d):
        z_copy_in = rdma(
            v["zst"].at[d], v["zin"].at[d], v["zss"].at[d], v["zrs"].at[d], {"sp": sp + 2 * NX * d}
        )
        z_copy_in.wait_recv()
        v["obuf"][tp] += v["zin"][d].astype(F32)

    def ag_copy(d):
        return rdma(
            v["obuf"].at[tp], v["obuf"].at[tp], v["ags"].at[d - 1], v["agr"].at[d - 1],
            at_y((tp + d) % NY),
        )

    for d in (1, 3, 2):
        ag_copy(d).start()

    @pl.loop(0, NZ)
    def _(i):
        @pl.when((i != z) | (c != z // 8))
        def _():
            rdma(
                v["kz"].at[0, 0], v["kzin"].at[i], v["kzs"].at[0, 0], v["kzr"].at[i],
                {"sp": i * 2 * NX + 2 * x + z // 8},
            ).wait_recv()

    total = v["kzin"][0].astype(F32)
    for i in range(1, NZ):
        total = total + v["kzin"][i].astype(F32)
    o_kw[...] = total

    for d in range(1, NY):
        yp = (tp + NY - d) % NY
        rdma(
            v["obuf"].at[yp], v["obuf"].at[yp], v["ags"].at[d - 1], v["agr"].at[d - 1], at_y(yp)
        ).wait_recv()
    out = v["obuf"][...].reshape(TOK, WIDE)
    o_lat[...] = out[:, :WIDTH]
    flip = out[:, WIDTH:].T
    o_krot[...] = jnp.where(x % 2 == 0, flip[:RDIM], flip[RDIM:])

    for n, name in enumerate(shared):
        share(n, name).wait_send()
    @pl.loop(1, zz + 1)
    def _(g):
        for xp in (near, side):
            for cp in x_keys(g, xp):
                cp.wait_send()
        for i in range(2):
            for cp in pass_on(g, i):
                cp.wait_send()

    for xp in (near, side, far):
        @pl.when(xp >= 2 * xh)
        def _():
            for cp in x_keys(0, xp):
                cp.wait_send()

        kx_copy(xp).wait_send()

        @pl.loop(0, zz + 1)
        def _(g):
            @pl.when((g > 0) | (xp // 2 <= xh))
            def _():
                x_copy(g, xp).wait_send()

    @pl.loop(1, after + 1)
    def _(d):
        for cp in z_keys(d):
            cp.wait_send()

    @pl.loop(1, zz + 1)
    def _(g):
        z_copy(g).wait_send()

    @pl.loop(0, last + 1)
    def _(s):
        @pl.when(valid(s))
        def _():
            for d in range(1, NY):
                y_copy(s, d).wait_send()

    mix_copy.wait_send()
    rot_copy.wait_send()
    main_copy.wait_send()

    @pl.loop(0, 8)
    def _(zp):
        for cp in range(2):
            @pl.when((8 * c + zp != z) | (c != cp))
            def _():
                kz_copy(zp, cp).wait_send()

    for d in range(1, NY):
        ag_copy(d).wait_send()


def store(*refs):
    *pairs, sem = refs
    count = len(pairs) // 2
    copies = [
        pltpu.make_async_copy(pairs[n], pairs[count + n], sem.at[n]) for n in range(count)
    ]
    for cp in copies:
        cp.start()
    for cp in copies:
        cp.wait()


def per_device(qm, qr, lat, rot, kw, vw, ho, og, logs):
    args = (qm, qr, lat, rot.T, kw, vw, ho, og, logs)
    shapes = (
        (TOK, HEADS * DIM), (TOK, HEADS * RDIM), (TOK, WIDTH), (RDIM, TOK), (PART, HEADS * DIM),
    )
    results = sum(4 * math.prod(s) for s in shapes)
    vmem = pl.BlockSpec(memory_space=pltpu.VMEM)
    hbm = pl.BlockSpec(memory_space=pltpu.HBM)
    held = pl.pallas_call(
        kernel,
        out_shape=[pltpu.VMEM(s, F32) for s in shapes],
        in_specs=[hbm] * len(args),
        out_specs=[vmem] * len(shapes),
        scratch_shapes=list(SCRATCH.values()),
        compiler_params=pltpu.CompilerParams(
            collective_id=0, has_side_effects=True, vmem_limit_bytes=VMEM_BYTES - results - (16 << 10)
        ),
        name="latent_attention_backward",
    )(*args)
    main, rotary, lat_out, rot_out, weight = pl.pallas_call(
        store,
        out_shape=[jax.ShapeDtypeStruct(s, F32) for s in shapes],
        in_specs=[vmem] * len(shapes),
        out_specs=[hbm] * len(shapes),
        scratch_shapes=[DMA((len(shapes),))],
        compiler_params=pltpu.CompilerParams(vmem_limit_bytes=4 << 20),
        name="store_outputs",
    )(*held)
    return main, rotary, lat_out, rot_out.T, weight


def solution(mesh):
    return jax.shard_map(
        per_device,
        mesh=mesh,
        in_specs=(
            P("sp", "tp"),
            P("sp", "tp"),
            P("sp", None),
            P("sp", None),
            P(None, "tp"),
            P(None, "tp"),
            P("sp", "tp"),
            P("sp", "tp"),
            P("tp", "sp"),
        ),
        out_specs=(P("sp", "tp"), P("sp", "tp"), P("sp", None), P("sp", None), P("sp", "tp")),
        check_vma=False,
    )
```

```python
import functools
import math

import jax
import jax.numpy as jnp
from jax import lax
from jax.experimental import pallas as pl
from jax.experimental.pallas import tpu as pltpu
from jax.sharding import PartitionSpec as P

VMEM_BYTES = 67043328
MESH = pl.DeviceIdType.MESH
F32 = jnp.float32
BF16 = jnp.bfloat16
NX = 4
NY = 4
NZ = 16
SPAN = 4
TOK = 128
HEADS = 4
DIM = 128
RDIM = 64
WIDTH = 512
ROWS = 2 * HEADS * TOK
QUART = TOK // NY
WIDE = WIDTH + 128
PAIR = 2 * WIDTH + 128
STEPS = 2 * SPAN
SLOTS = 4
PART = 4
FACTOR = (DIM + RDIM) ** (-0.5)

DMA = pltpu.SemaphoreType.DMA


def dot(a, b, ca, cb, precision=None):
    return lax.dot_general(
        a, b, (((ca,), (cb,)), ((), ())), preferred_element_type=F32, precision=precision
    )


SCRATCH = dict(
    klat=pltpu.VMEM((SPAN, NX, TOK, WIDTH), BF16),
    krot=pltpu.VMEM((SPAN, NX, RDIM, TOK), BF16),
    qm=pltpu.VMEM((2, TOK, HEADS * DIM), BF16),
    og=pltpu.VMEM((2, TOK, HEADS * DIM), BF16),
    ho=pltpu.VMEM((2, TOK, HEADS * DIM), BF16),
    qr=pltpu.VMEM((2, TOK, HEADS * RDIM), BF16),
    lg=pltpu.VMEM((2, HEADS, TOK), F32),
    kw=pltpu.VMEM((WIDTH, HEADS * DIM), BF16),
    vw=pltpu.VMEM((WIDTH, HEADS * DIM), BF16),
    ql=pltpu.VMEM((ROWS, WIDTH), BF16),
    gr=pltpu.VMEM((ROWS, WIDTH), BF16),
    qrd=pltpu.VMEM((ROWS, 128), BF16),
    trow=pltpu.VMEM((1, ROWS), F32),
    lrow=pltpu.VMEM((1, ROWS), F32),
    mixed=pltpu.VMEM((ROWS, WIDTH), F32),
    rsum=pltpu.VMEM((ROWS, RDIM), F32),
    gf=pltpu.VMEM((SLOTS, NY, QUART, PAIR), F32),
    gst=pltpu.VMEM((STEPS, NY, QUART, PAIR), BF16),
    yin=pltpu.VMEM((STEPS, NY - 1, QUART, PAIR), BF16),
    xacc=pltpu.VMEM((SPAN, QUART, WIDE), F32),
    xst=pltpu.VMEM((SPAN, NX, QUART, WIDE), BF16),
    xin=pltpu.VMEM((SPAN, NX, QUART, WIDE), BF16),
    zst=pltpu.VMEM((SPAN, QUART, WIDE), BF16),
    zin=pltpu.VMEM((SPAN, QUART, WIDE), BF16),
    facc=pltpu.VMEM((QUART, WIDE), F32),
    obuf=pltpu.VMEM((NY, QUART, WIDE), F32),
    mrecv=pltpu.VMEM((ROWS, WIDTH // 2), F32),
    ml=pltpu.VMEM((ROWS, WIDTH // 2), BF16),
    rrecv=pltpu.VMEM((ROWS // 2, RDIM), F32),
    osend=pltpu.VMEM((TOK, HEADS * DIM), F32),
    orecv=pltpu.VMEM((TOK, HEADS * DIM), F32),
    kf=pltpu.VMEM((NX, 8, 8, HEADS * DIM), F32),
    kst=pltpu.VMEM((NX, 8, 8, HEADS * DIM), BF16),
    kxin=pltpu.VMEM((NX, 8, 8, HEADS * DIM), BF16),
    kz=pltpu.VMEM((8, 2, PART, HEADS * DIM), BF16),
    kzin=pltpu.VMEM((NZ, PART, HEADS * DIM), BF16),
    insem=DMA((9,)),
    qss=DMA((5,)), qrs=DMA((5,)),
    zks=DMA((SPAN, 2)), zkr=DMA((SPAN, 2)),
    xks=DMA((SPAN, NX, 2)), xkr=DMA((SPAN, NX, 2)),
    yss=DMA((STEPS, NY - 1)), yrs=DMA((STEPS, NY - 1)),
    fks=DMA((SPAN, 2, 2)), fkr=DMA((SPAN, 2, 2)),
    far=pltpu.SemaphoreType.REGULAR((3,)),
    xss=DMA((SPAN, NX)), xrs=DMA((SPAN, NX)),
    zss=DMA((SPAN,)), zrs=DMA((SPAN,)),
    mss=DMA((3,)), mrs=DMA((3,)),
    kxs=DMA((NX,)), kxr=DMA((NX,)),
    kzs=DMA((8, 2)), kzr=DMA((NZ,)),
    ags=DMA((NY - 1,)), agr=DMA((NY - 1,)),
)
NAMES = tuple(SCRATCH)


def rdma(src, dst, ss, rs, dev):
    return pltpu.make_async_remote_copy(
        src_ref=src, dst_ref=dst, send_sem=ss, recv_sem=rs, device_id=dev, device_id_type=MESH
    )


def kernel(qm_h, qr_h, lat_h, rot_h, kw_h, vw_h, ho_h, og_h, lg_h,
           o_main, o_rot, o_lat, o_krot, o_kw, *scratch):
    v = dict(zip(NAMES, scratch))
    klat, krot, ql, gr, qrd = v["klat"], v["krot"], v["ql"], v["gr"], v["qrd"]
    mixed, rsum, gf, gst, yin = v["mixed"], v["rsum"], v["gf"], v["gst"], v["yin"]
    trow, lrow = v["trow"], v["lrow"]
    sp = lax.axis_index("sp")
    tp = lax.axis_index("tp")
    z = sp // (2 * NX)
    x = (sp // 2) % NX
    c = sp % 2
    other = 1 - c
    xh = x // 2
    near = x + 1 - 2 * (x % 2)
    far = (x + 2) % NX
    side = NX - 1 - x
    seq = (z + 1) // SPAN
    zz = z - jnp.maximum(seq * SPAN - 1, 0)
    after = jnp.minimum(seq * SPAN + SPAN - 1, NZ) - 1 - z
    partner = {"sp": sp + 1 - 2 * c}

    def at_x(xp):
        return {"sp": sp + 2 * (xp - x)}

    def at_y(yp):
        return {"tp": yp}

    barrier = pltpu.get_barrier_semaphore()

    def at_z(d, cp):
        return {"sp": ((z + NZ + d) % NZ) * 2 * NX + 2 * x + cp}

    for d in (1, -1):
        for cp in range(2):
            pl.semaphore_signal(barrier, inc=1, device_id=at_z(d, cp), device_id_type=MESH)
    pl.semaphore_signal(barrier, inc=1, device_id=partner, device_id_type=MESH)
    for d in range(1, NX):
        pl.semaphore_signal(barrier, inc=1, device_id=at_x((x + d) % NX), device_id_type=MESH)
    for d in range(1, NY):
        pl.semaphore_signal(barrier, inc=1, device_id=at_y((tp + d) % NY), device_id_type=MESH)

    shared = ("qm", "og", "ho", "qr", "lg")
    sources = (qm_h, og_h, ho_h, qr_h, lg_h)
    loads = [
        pltpu.make_async_copy(lat_h, klat.at[0, x], v["insem"].at[0]),
        pltpu.make_async_copy(rot_h, krot.at[0, x], v["insem"].at[1]),
    ]
    loads += [
        pltpu.make_async_copy(src, v[name].at[c], v["insem"].at[2 + n])
        for n, (name, src) in enumerate(zip(shared, sources))
    ]
    loads += [
        pltpu.make_async_copy(kw_h, v["kw"], v["insem"].at[7]),
        pltpu.make_async_copy(vw_h, v["vw"], v["insem"].at[8]),
    ]
    for cp in loads:
        cp.start()
    mixed[...] = jnp.zeros_like(mixed)
    rsum[...] = jnp.zeros_like(rsum)
    for cp in loads:
        cp.wait()

    def prepare(b):
        for h in range(HEADS):
            start = pl.multiple_of(b * (HEADS * TOK) + h * TOK, TOK)
            rows = pl.ds(start, TOK)
            cols = slice(h * DIM, (h + 1) * DIM)
            ql[rows] = dot(v["qm"][b, :, cols], v["kw"][:, cols], 1, 1).astype(BF16)
            og = v["og"][b, :, cols]
            gr[rows] = dot(og, v["vw"][:, cols], 1, 1).astype(BF16)
            rot = v["qr"][b, :, h * RDIM : (h + 1) * RDIM]
            qrd[rows] = jnp.concatenate([rot, rot], axis=1)
            prod = v["ho"][b, :, cols].astype(F32) * og.astype(F32)
            trow[:, rows] = dot(jnp.ones((8, DIM), F32), prod, 1, 1, lax.Precision.HIGHEST)[0:1]
            lrow[:, rows] = v["lg"][b, h : h + 1, :]

    def share(n, name):
        return rdma(v[name].at[c], v[name].at[c], v["qss"].at[n], v["qrs"].at[n], partner)

    def share_in(n, name):
        return rdma(v[name].at[other], v[name].at[other], v["qss"].at[n], v["qrs"].at[n], partner)

    keys = (klat, krot)

    def x_keys(g, xp):
        return [
            rdma(k.at[g, x], k.at[g, x], v["xks"].at[g, xp, n], v["xkr"].at[g, x, n], at_x(xp))
            for n, k in enumerate(keys)
        ]

    def x_keys_in(g, xp):
        return [
            rdma(k.at[g, xp], k.at[g, xp], v["xks"].at[g, xp, n], v["xkr"].at[g, xp, n], at_x(xp))
            for n, k in enumerate(keys)
        ]

    prepare(c)
    pl.semaphore_wait(barrier, 4 + 1 + NX - 1 + NY - 1)

    def greet(n):
        for d in (1, -1):
            pl.semaphore_signal(
                v["far"].at[n], inc=1, device_id=at_z(d << n, c), device_id_type=MESH
            )

    def met(n):
        pl.semaphore_wait(v["far"].at[n], 2)

    greet(0)

    for n, name in enumerate(shared):
        share(n, name).start()

    def lift(d):
        return [
            rdma(
                k.at[d - 1, x], k.at[d, x], v["zks"].at[d, n], v["zkr"].at[d, n],
                {"sp": sp + 2 * NX},
            )
            for n, k in enumerate(keys)
        ]

    def send_up(d):
        @pl.when((after > 0) & (d < SPAN))
        def _():
            for cp in lift(d):
                cp.start()

    send_up(1)
    for xp in (near, side, far):
        @pl.when(xp >= 2 * xh)
        def _():
            for cp in x_keys(0, xp):
                cp.start()

    for n, name in enumerate(shared):
        share_in(n, name).wait_recv()
    prepare(other)
    met(0)
    greet(1)

    def forward(g):
        @pl.when(g <= zz)
        def _():
            for cp in lift(g):
                cp.wait_recv()
            send_up(g + 1)
            for xp in (near, side):
                for cp in x_keys(g, xp):
                    cp.start()

    last = 2 * zz + 1

    def pass_on(g, i):
        src, dst = ((near, side), (side, near))[i]
        out = []
        for n, (k, size) in enumerate(((klat, TOK // 2), (krot, RDIM // 2))):
            part = k.at[g, src, pl.ds(i * size, size)]
            out.append(
                rdma(part, part, v["fks"].at[g, i, n], v["fkr"].at[g, i, n], at_x(dst))
            )
        return out

    def passed_in(g, i):
        out = []
        for n, (k, size) in enumerate(((klat, TOK // 2), (krot, RDIM // 2))):
            part = k.at[g, far, pl.ds(i * size, size)]
            out.append(
                rdma(part, part, v["fks"].at[g, i, n], v["fkr"].at[g, i, n], at_x((near, side)[1 - i]))
            )
        return out

    def pair_of(s):
        return xh + (s % 2) * (1 - 2 * xh)

    def valid(s):
        return (s >= 0) & (s <= last) & ((s != 1) | (xh == 1))

    def y_copy(s, d):
        return rdma(
            gst.at[s, (tp + d) % NY], yin.at[s, d - 1], v["yss"].at[s, d - 1], v["yrs"].at[s, d - 1],
            at_y((tp + d) % NY),
        )

    def attend(s):
        g = s // 2
        m = pair_of(s)

        @pl.when(s % 2 == 0)
        def _():
            for cp in x_keys_in(g, near):
                cp.wait_recv()

            @pl.when(g > 0)
            def _():
                for cp in x_keys_in(g, side):
                    cp.wait_recv()
                for i in range(2):
                    for cp in pass_on(g, i):
                        cp.start()
                forward(g + 1)

        @pl.when((s % 2 == 1) & (g > 0))
        def _():
            for i in range(2):
                for cp in passed_in(g, i):
                    cp.wait_recv()

        @pl.when(s == 1)
        def _():
            for xp in (side, far):
                for cp in x_keys_in(0, xp):
                    cp.wait_recv()

        lt = klat[g, pl.ds(2 * m, 2)].reshape(2 * TOK, WIDTH)
        rt = jnp.concatenate([krot[g, 2 * m], krot[g, 2 * m + 1]], axis=1)
        scores = dot(lt, ql[...], 1, 1) + dot(rt, qrd[:, :RDIM], 0, 1)
        weights = jnp.exp(FACTOR * scores - lrow[...])
        k_id = lax.broadcasted_iota(jnp.int32, (2 * TOK, 1), 0)
        k_pos = (2 * m + k_id // TOK) * (2 * TOK) + c * TOK + k_id % TOK
        k_pos = jnp.where(g > 0, -1, k_pos)
        q_id = lax.broadcasted_iota(jnp.int32, (1, ROWS), 1)
        q_pos = (2 * x + q_id // (HEADS * TOK)) * TOK + q_id % TOK
        weights = jnp.where(k_pos <= q_pos, weights, 0.0)
        slopes = dot(lt, gr[...], 1, 1)
        dscores = weights * (slopes - trow[...])
        wl = weights.astype(BF16)
        dl = dscores.astype(BF16)
        grad = FACTOR * dot(dl, ql[...], 1, 0) + dot(wl, gr[...], 1, 0)
        slot = s % SLOTS
        gf[slot, :, :, :WIDTH] = grad[:TOK].reshape(NY, QUART, WIDTH)
        gf[slot, :, :, WIDTH : 2 * WIDTH] = grad[TOK:].reshape(NY, QUART, WIDTH)
        rgrad = FACTOR * dot(dl, qrd[...], 1, 0)
        lane = lax.broadcasted_iota(jnp.int32, (TOK, 128), 1)
        packed = jnp.where(lane < RDIM, rgrad[:TOK], rgrad[TOK:])
        gf[slot, :, :, 2 * WIDTH :] = packed.reshape(NY, QUART, 128)
        gst[s] = gf[slot].astype(BF16)
        for d in (1, 3, 2):
            y_copy(s, d).start()
        mixed[...] += dot(dl, lt, 0, 0)
        rsum[...] += dot(dl, rt, 0, 1)

    def x_copy(g, xp):
        return rdma(
            v["xst"].at[g, xp], v["xin"].at[g, x], v["xss"].at[g, xp], v["xrs"].at[g, x], at_x(xp)
        )

    def x_copy_in(g, xp):
        return rdma(
            v["xst"].at[g, xp], v["xin"].at[g, xp], v["xss"].at[g, xp], v["xrs"].at[g, xp], at_x(xp)
        )

    def reduce_y(s):
        @pl.when(valid(s))
        def _():
            g = s // 2
            m = pair_of(s)
            total = gf[s % SLOTS, tp]
            for d in range(1, NY):
                y_copy(s, d).wait_recv()
                total = total + yin[s, d - 1].astype(F32)
            for b in range(2):
                xp = 2 * m + b
                lat = total[:, b * WIDTH : (b + 1) * WIDTH]
                rot = total[:, 2 * WIDTH :]

                @pl.when(xp == x)
                def _():
                    v["xacc"][g, :, :WIDTH] = lat
                    v["xacc"][g, :, WIDTH:] = rot

                @pl.when(xp != x)
                def _():
                    v["xst"][g, xp, :, :WIDTH] = lat.astype(BF16)
                    v["xst"][g, xp, :, WIDTH:] = rot.astype(BF16)
                    x_copy(g, xp).start()

    def z_copy(g):
        return rdma(
            v["zst"].at[g], v["zin"].at[g], v["zss"].at[g], v["zrs"].at[g], {"sp": sp - 2 * NX * g}
        )

    def reduce_x(s):
        @pl.when((s >= 0) & (s <= last) & (s % 2 == 1))
        def _():
            g = s // 2
            v["facc"][...] = v["xacc"][g]
            for d in range(1, NX):
                xp = (x + d) % NX

                @pl.when((g > 0) | (xp >= 2 * xh))
                def _():
                    x_copy_in(g, xp).wait_recv()
                    v["facc"][...] += v["xin"][g, xp].astype(F32)

            @pl.when(g > 0)
            def _():
                v["zst"][g] = v["facc"][...].astype(BF16)
                z_copy(g).start()

            @pl.when(g == 0)
            def _():
                v["obuf"][tp] = v["facc"][...]

    @pl.loop(0, last + 1)
    def _(s):
        @pl.when(valid(s))
        def _():
            attend(s)

        @pl.when(s == 0)
        def _():
            forward(1)

        @pl.when(s == 0)
        def _():
            met(1)
            greet(2)

        reduce_y(s - 2)
        reduce_x(s - 3)

    half = WIDTH // 2
    mine = pl.ds(pl.multiple_of(half * c, half), half)
    theirs = pl.ds(pl.multiple_of(half * other, half), half)
    my_rows = pl.ds(pl.multiple_of(c * (ROWS // 2), ROWS // 2), ROWS // 2)
    their_rows = pl.ds(pl.multiple_of(other * (ROWS // 2), ROWS // 2), ROWS // 2)
    mix_copy = rdma(mixed.at[:, theirs], v["mrecv"], v["mss"].at[0], v["mrs"].at[0], partner)
    rot_copy = rdma(rsum.at[their_rows], v["rrecv"], v["mss"].at[1], v["mrs"].at[1], partner)
    main_copy = rdma(v["osend"], v["orecv"], v["mss"].at[2], v["mrs"].at[2], partner)
    mix_copy.start()
    rot_copy.start()
    mix_copy.wait_recv()
    ml = v["ml"]
    ml[...] = (mixed[:, mine] + v["mrecv"][...]).astype(BF16)

    def main_part(b, h):
        rows = pl.ds(pl.multiple_of(b * (HEADS * TOK) + h * TOK, TOK), TOK)
        return dot(ml[rows], v["kw"][mine, h * DIM : (h + 1) * DIM], 1, 0)

    for h in range(HEADS):
        cols = slice(h * DIM, (h + 1) * DIM)
        left = jnp.concatenate(
            [ml[b * HEADS * TOK + h * TOK : b * HEADS * TOK + (h + 1) * TOK] for b in range(2)], axis=0
        )
        right = jnp.concatenate([v["qm"][b, :, cols] for b in range(2)], axis=0)
        term = (FACTOR * dot(left, right, 0, 0)).reshape(8, NX, 8, DIM)
        for xp in range(NX):
            v["kf"][xp, :, :, cols] = term[:, xp]
            v["kst"][xp, :, :, cols] = term[:, xp].astype(BF16)

    def kx_copy(xp):
        return rdma(v["kst"].at[xp], v["kxin"].at[x], v["kxs"].at[xp], v["kxr"].at[x], at_x(xp))

    def kx_copy_in(xp):
        return rdma(v["kst"].at[xp], v["kxin"].at[xp], v["kxs"].at[xp], v["kxr"].at[xp], at_x(xp))

    for d in (1, 3, 2):
        kx_copy((x + d) % NX).start()

    for h in range(HEADS):
        v["osend"][:, h * DIM : (h + 1) * DIM] = main_part(other, h)
    main_copy.start()
    reduce_y(last - 1)
    reduce_x(last - 2)
    reduce_y(last)

    total = v["kf"][x]
    for d in range(1, NX):
        xp = (x + d) % NX
        kx_copy_in(xp).wait_recv()
        total = total + v["kxin"][xp].astype(F32)
    total = total.astype(BF16)
    v["kz"][:, 0] = total[:, :PART]
    v["kz"][:, 1] = total[:, PART:]

    def kz_copy(zp, cp):
        return rdma(
            v["kz"].at[zp, cp], v["kzin"].at[z], v["kzs"].at[zp, cp], v["kzr"].at[z],
            {"sp": (8 * c + zp) * 2 * NX + 2 * x + cp},
        )

    met(2)

    @pl.loop(0, 8)
    def _(i):
        zp = (z + i) % 8
        for cp in range(2):
            here = (8 * c + zp == z) & (c == cp)

            @pl.when(jnp.logical_not(here))
            def _():
                kz_copy(zp, cp).start()

            @pl.when(here)
            def _():
                v["kzin"][z] = v["kz"][zp, cp]

    reduce_x(last)
    rot_copy.wait_recv()
    for h in range(HEADS):
        rows = pl.ds(pl.multiple_of(c * (HEADS * TOK) + h * TOK, TOK), TOK)
        o_rot[:, h * RDIM : (h + 1) * RDIM] = FACTOR * (
            rsum[rows] + v["rrecv"][h * TOK : (h + 1) * TOK]
        )
    main_copy.wait_recv()
    for h in range(HEADS):
        cols = slice(h * DIM, (h + 1) * DIM)
        o_main[:, cols] = FACTOR * (main_part(c, h) + v["orecv"][:, cols])

    @pl.loop(1, after + 1)
    def _(d):
        z_copy_in = rdma(
            v["zst"].at[d], v["zin"].at[d], v["zss"].at[d], v["zrs"].at[d], {"sp": sp + 2 * NX * d}
        )
        z_copy_in.wait_recv()
        v["obuf"][tp] += v["zin"][d].astype(F32)

    def ag_copy(d):
        return rdma(
            v["obuf"].at[tp], v["obuf"].at[tp], v["ags"].at[d - 1], v["agr"].at[d - 1],
            at_y((tp + d) % NY),
        )

    for d in (1, 3, 2):
        ag_copy(d).start()

    @pl.loop(0, NZ)
    def _(i):
        @pl.when((i != z) | (c != z // 8))
        def _():
            rdma(
                v["kz"].at[0, 0], v["kzin"].at[i], v["kzs"].at[0, 0], v["kzr"].at[i],
                {"sp": i * 2 * NX + 2 * x + z // 8},
            ).wait_recv()

    total = v["kzin"][0].astype(F32)
    for i in range(1, NZ):
        total = total + v["kzin"][i].astype(F32)
    o_kw[...] = total

    for d in range(1, NY):
        yp = (tp + NY - d) % NY
        rdma(
            v["obuf"].at[yp], v["obuf"].at[yp], v["ags"].at[d - 1], v["agr"].at[d - 1], at_y(yp)
        ).wait_recv()
    out = v["obuf"][...].reshape(TOK, WIDE)
    o_lat[...] = out[:, :WIDTH]
    flip = out[:, WIDTH:].T
    o_krot[...] = jnp.where(x % 2 == 0, flip[:RDIM], flip[RDIM:])

    for n, name in enumerate(shared):
        share(n, name).wait_send()
    @pl.loop(1, zz + 1)
    def _(g):
        for xp in (near, side):
            for cp in x_keys(g, xp):
                cp.wait_send()
        for i in range(2):
            for cp in pass_on(g, i):
                cp.wait_send()

    for xp in (near, side, far):
        @pl.when(xp >= 2 * xh)
        def _():
            for cp in x_keys(0, xp):
                cp.wait_send()

        kx_copy(xp).wait_send()

        @pl.loop(0, zz + 1)
        def _(g):
            @pl.when((g > 0) | (xp // 2 <= xh))
            def _():
                x_copy(g, xp).wait_send()

    @pl.when(after > 0)
    def _():
        @pl.loop(1, zz + 2)
        def _(d):
            for cp in lift(d):
                cp.wait_send()

    @pl.loop(1, zz + 1)
    def _(g):
        z_copy(g).wait_send()

    @pl.loop(0, last + 1)
    def _(s):
        @pl.when(valid(s))
        def _():
            for d in range(1, NY):
                y_copy(s, d).wait_send()

    mix_copy.wait_send()
    rot_copy.wait_send()
    main_copy.wait_send()

    @pl.loop(0, 8)
    def _(zp):
        for cp in range(2):
            @pl.when((8 * c + zp != z) | (c != cp))
            def _():
                kz_copy(zp, cp).wait_send()

    for d in range(1, NY):
        ag_copy(d).wait_send()


def store(*refs):
    *pairs, sem = refs
    count = len(pairs) // 2
    copies = [
        pltpu.make_async_copy(pairs[n], pairs[count + n], sem.at[n]) for n in range(count)
    ]
    for cp in copies:
        cp.start()
    for cp in copies:
        cp.wait()


def per_device(qm, qr, lat, rot, kw, vw, ho, og, logs):
    args = (qm, qr, lat, rot.T, kw, vw, ho, og, logs)
    shapes = (
        (TOK, HEADS * DIM), (TOK, HEADS * RDIM), (TOK, WIDTH), (RDIM, TOK), (PART, HEADS * DIM),
    )
    results = sum(4 * math.prod(s) for s in shapes)
    vmem = pl.BlockSpec(memory_space=pltpu.VMEM)
    hbm = pl.BlockSpec(memory_space=pltpu.HBM)
    held = pl.pallas_call(
        kernel,
        out_shape=[pltpu.VMEM(s, F32) for s in shapes],
        in_specs=[hbm] * len(args),
        out_specs=[vmem] * len(shapes),
        scratch_shapes=list(SCRATCH.values()),
        compiler_params=pltpu.CompilerParams(
            collective_id=0, has_side_effects=True, vmem_limit_bytes=VMEM_BYTES - results - (16 << 10)
        ),
        name="latent_attention_backward",
    )(*args)
    main, rotary, lat_out, rot_out, weight = pl.pallas_call(
        store,
        out_shape=[jax.ShapeDtypeStruct(s, F32) for s in shapes],
        in_specs=[vmem] * len(shapes),
        out_specs=[hbm] * len(shapes),
        scratch_shapes=[DMA((len(shapes),))],
        compiler_params=pltpu.CompilerParams(vmem_limit_bytes=4 << 20),
        name="store_outputs",
    )(*held)
    return main, rotary, lat_out, rot_out.T, weight


def solution(mesh):
    return jax.shard_map(
        per_device,
        mesh=mesh,
        in_specs=(
            P("sp", "tp"),
            P("sp", "tp"),
            P("sp", None),
            P("sp", None),
            P(None, "tp"),
            P(None, "tp"),
            P("sp", "tp"),
            P("sp", "tp"),
            P("tp", "sp"),
        ),
        out_specs=(P("sp", "tp"), P("sp", "tp"), P("sp", None), P("sp", None), P("sp", "tp")),
        check_vma=False,
    )
```

```python
import functools
import math

import jax
import jax.numpy as jnp
from jax import lax
from jax.experimental import pallas as pl
from jax.experimental.pallas import tpu as pltpu
from jax.sharding import PartitionSpec as P

VMEM_BYTES = 67043328
MESH = pl.DeviceIdType.MESH
F32 = jnp.float32
BF16 = jnp.bfloat16
NX = 4
NY = 4
NZ = 16
SPAN = 4
TOK = 128
HEADS = 4
DIM = 128
RDIM = 64
WIDTH = 512
ROWS = 2 * HEADS * TOK
QUART = TOK // NY
WIDE = WIDTH + 128
PAIR = 2 * WIDTH + 128
STEPS = 2 * SPAN
SLOTS = 4
PART = 4
FACTOR = (DIM + RDIM) ** (-0.5)

DMA = pltpu.SemaphoreType.DMA


def dot(a, b, ca, cb, precision=None):
    return lax.dot_general(
        a, b, (((ca,), (cb,)), ((), ())), preferred_element_type=F32, precision=precision
    )


SCRATCH = dict(
    klat=pltpu.VMEM((SPAN, NX, TOK, WIDTH), BF16),
    krot=pltpu.VMEM((SPAN, NX, RDIM, TOK), BF16),
    qm=pltpu.VMEM((2, TOK, HEADS * DIM), BF16),
    og=pltpu.VMEM((2, TOK, HEADS * DIM), BF16),
    ho=pltpu.VMEM((2, TOK, HEADS * DIM), BF16),
    qr=pltpu.VMEM((2, TOK, HEADS * RDIM), BF16),
    lg=pltpu.VMEM((2, HEADS, TOK), F32),
    kw=pltpu.VMEM((WIDTH, HEADS * DIM), BF16),
    vw=pltpu.VMEM((WIDTH, HEADS * DIM), BF16),
    ql=pltpu.VMEM((ROWS, WIDTH), BF16),
    gr=pltpu.VMEM((ROWS, WIDTH), BF16),
    qrd=pltpu.VMEM((ROWS, 128), BF16),
    trow=pltpu.VMEM((1, ROWS), F32),
    lrow=pltpu.VMEM((1, ROWS), F32),
    mixed=pltpu.VMEM((ROWS, WIDTH), F32),
    rsum=pltpu.VMEM((ROWS, RDIM), F32),
    gf=pltpu.VMEM((SLOTS, NY, QUART, PAIR), F32),
    gst=pltpu.VMEM((STEPS, NY, QUART, PAIR), BF16),
    yin=pltpu.VMEM((STEPS, NY - 1, QUART, PAIR), BF16),
    xacc=pltpu.VMEM((SPAN, QUART, WIDE), F32),
    xst=pltpu.VMEM((SPAN, NX, QUART, WIDE), BF16),
    xin=pltpu.VMEM((SPAN, NX, QUART, WIDE), BF16),
    zst=pltpu.VMEM((SPAN, QUART, WIDE), BF16),
    zin=pltpu.VMEM((SPAN, QUART, WIDE), BF16),
    facc=pltpu.VMEM((QUART, WIDE), F32),
    obuf=pltpu.VMEM((NY, QUART, WIDE), F32),
    mrecv=pltpu.VMEM((ROWS, WIDTH // 2), F32),
    ml=pltpu.VMEM((ROWS, WIDTH // 2), BF16),
    rrecv=pltpu.VMEM((ROWS // 2, RDIM), F32),
    osend=pltpu.VMEM((TOK, HEADS * DIM), F32),
    orecv=pltpu.VMEM((TOK, HEADS * DIM), F32),
    kf=pltpu.VMEM((NX, 8, 8, HEADS * DIM), F32),
    kst=pltpu.VMEM((NX, 8, 8, HEADS * DIM), BF16),
    kxin=pltpu.VMEM((NX, 8, 8, HEADS * DIM), BF16),
    kz=pltpu.VMEM((8, 2, PART, HEADS * DIM), BF16),
    kzin=pltpu.VMEM((NZ, PART, HEADS * DIM), BF16),
    insem=DMA((9,)),
    qss=DMA((5,)), qrs=DMA((5,)),
    zks=DMA((SPAN, 2)), zkr=DMA((SPAN, 2)),
    xks=DMA((SPAN, NX, 2)), xkr=DMA((SPAN, NX, 2)),
    yss=DMA((STEPS, NY - 1)), yrs=DMA((STEPS, NY - 1)),
    fks=DMA((SPAN, 2, 2)), fkr=DMA((SPAN, 2, 2)),
    far=pltpu.SemaphoreType.REGULAR((3,)),
    xss=DMA((SPAN, NX)), xrs=DMA((SPAN, NX)),
    zss=DMA((SPAN,)), zrs=DMA((SPAN,)),
    mss=DMA((3,)), mrs=DMA((3,)),
    kxs=DMA((NX,)), kxr=DMA((NX,)),
    kzs=DMA((8, 2)), kzr=DMA((NZ,)),
    ags=DMA((NY - 1,)), agr=DMA((NY - 1,)),
)
NAMES = tuple(SCRATCH)


def rdma(src, dst, ss, rs, dev):
    return pltpu.make_async_remote_copy(
        src_ref=src, dst_ref=dst, send_sem=ss, recv_sem=rs, device_id=dev, device_id_type=MESH
    )


def kernel(qm_h, qr_h, lat_h, rot_h, kw_h, vw_h, ho_h, og_h, lg_h,
           o_main, o_rot, o_lat, o_krot, o_kw, *scratch):
    v = dict(zip(NAMES, scratch))
    klat, krot, ql, gr, qrd = v["klat"], v["krot"], v["ql"], v["gr"], v["qrd"]
    mixed, rsum, gf, gst, yin = v["mixed"], v["rsum"], v["gf"], v["gst"], v["yin"]
    trow, lrow = v["trow"], v["lrow"]
    sp = lax.axis_index("sp")
    tp = lax.axis_index("tp")
    z = sp // (2 * NX)
    x = (sp // 2) % NX
    c = sp % 2
    other = 1 - c
    xh = x // 2
    near = x + 1 - 2 * (x % 2)
    far = (x + 2) % NX
    side = NX - 1 - x
    seq = (z + 1) // SPAN
    zz = z - jnp.maximum(seq * SPAN - 1, 0)
    after = jnp.minimum(seq * SPAN + SPAN - 1, NZ) - 1 - z
    partner = {"sp": sp + 1 - 2 * c}

    def at_x(xp):
        return {"sp": sp + 2 * (xp - x)}

    def at_y(yp):
        return {"tp": yp}

    barrier = pltpu.get_barrier_semaphore()

    def at_z(d, cp):
        return {"sp": ((z + NZ + d) % NZ) * 2 * NX + 2 * x + cp}

    for d in (1, -1):
        for cp in range(2):
            pl.semaphore_signal(barrier, inc=1, device_id=at_z(d, cp), device_id_type=MESH)
    pl.semaphore_signal(barrier, inc=1, device_id=partner, device_id_type=MESH)
    for d in range(1, NX):
        pl.semaphore_signal(barrier, inc=1, device_id=at_x((x + d) % NX), device_id_type=MESH)
    for d in range(1, NY):
        pl.semaphore_signal(barrier, inc=1, device_id=at_y((tp + d) % NY), device_id_type=MESH)

    shared = ("qm", "og", "ho", "qr", "lg")
    sources = (qm_h, og_h, ho_h, qr_h, lg_h)
    loads = [
        pltpu.make_async_copy(lat_h, klat.at[0, x], v["insem"].at[0]),
        pltpu.make_async_copy(rot_h, krot.at[0, x], v["insem"].at[1]),
    ]
    loads += [
        pltpu.make_async_copy(src, v[name].at[c], v["insem"].at[2 + n])
        for n, (name, src) in enumerate(zip(shared, sources))
    ]
    loads += [
        pltpu.make_async_copy(kw_h, v["kw"], v["insem"].at[7]),
        pltpu.make_async_copy(vw_h, v["vw"], v["insem"].at[8]),
    ]
    for cp in loads:
        cp.start()
    mixed[...] = jnp.zeros_like(mixed)
    rsum[...] = jnp.zeros_like(rsum)
    for cp in loads:
        cp.wait()

    def prepare(b):
        for h in range(HEADS):
            start = pl.multiple_of(b * (HEADS * TOK) + h * TOK, TOK)
            rows = pl.ds(start, TOK)
            cols = slice(h * DIM, (h + 1) * DIM)
            ql[rows] = dot(v["qm"][b, :, cols], v["kw"][:, cols], 1, 1).astype(BF16)
            og = v["og"][b, :, cols]
            gr[rows] = dot(og, v["vw"][:, cols], 1, 1).astype(BF16)
            rot = v["qr"][b, :, h * RDIM : (h + 1) * RDIM]
            qrd[rows] = jnp.concatenate([rot, rot], axis=1)
            prod = v["ho"][b, :, cols].astype(F32) * og.astype(F32)
            trow[:, rows] = dot(jnp.ones((8, DIM), F32), prod, 1, 1, lax.Precision.HIGHEST)[0:1]
            lrow[:, rows] = v["lg"][b, h : h + 1, :]

    def share(n, name):
        return rdma(v[name].at[c], v[name].at[c], v["qss"].at[n], v["qrs"].at[n], partner)

    def share_in(n, name):
        return rdma(v[name].at[other], v[name].at[other], v["qss"].at[n], v["qrs"].at[n], partner)

    keys = (klat, krot)

    def x_keys(g, xp):
        return [
            rdma(k.at[g, x], k.at[g, x], v["xks"].at[g, xp, n], v["xkr"].at[g, x, n], at_x(xp))
            for n, k in enumerate(keys)
        ]

    def x_keys_in(g, xp):
        return [
            rdma(k.at[g, xp], k.at[g, xp], v["xks"].at[g, xp, n], v["xkr"].at[g, xp, n], at_x(xp))
            for n, k in enumerate(keys)
        ]

    prepare(c)
    pl.semaphore_wait(barrier, 4 + 1 + NX - 1 + NY - 1)

    def greet(n):
        for d in (1, -1):
            pl.semaphore_signal(
                v["far"].at[n], inc=1, device_id=at_z(d << n, c), device_id_type=MESH
            )

    def met(n):
        pl.semaphore_wait(v["far"].at[n], 2)

    greet(0)

    for n, name in enumerate(shared):
        share(n, name).start()

    def lift(d):
        return [
            rdma(
                k.at[d - 1, x], k.at[d, x], v["zks"].at[d, n], v["zkr"].at[d, n],
                {"sp": sp + 2 * NX},
            )
            for n, k in enumerate(keys)
        ]

    def send_up(d):
        @pl.when((after > 0) & (d < SPAN))
        def _():
            for cp in lift(d):
                cp.start()

    send_up(1)
    for xp in (near, side, far):
        @pl.when(xp >= 2 * xh)
        def _():
            for cp in x_keys(0, xp):
                cp.start()

    for n, name in enumerate(shared):
        share_in(n, name).wait_recv()
    prepare(other)
    met(0)
    greet(1)

    def forward(g):
        @pl.when(g <= zz)
        def _():
            for cp in lift(g):
                cp.wait_recv()
            send_up(g + 1)
            for xp in (near, side):
                for cp in x_keys(g, xp):
                    cp.start()

    last = 2 * zz + 1

    def pass_on(g, i):
        src, dst = ((near, side), (side, near))[i]
        out = []
        for n, (k, size) in enumerate(((klat, TOK // 2), (krot, RDIM // 2))):
            part = k.at[g, src, pl.ds(i * size, size)]
            out.append(
                rdma(part, part, v["fks"].at[g, i, n], v["fkr"].at[g, i, n], at_x(dst))
            )
        return out

    def passed_in(g, i):
        out = []
        for n, (k, size) in enumerate(((klat, TOK // 2), (krot, RDIM // 2))):
            part = k.at[g, far, pl.ds(i * size, size)]
            out.append(
                rdma(part, part, v["fks"].at[g, i, n], v["fkr"].at[g, i, n], at_x((near, side)[1 - i]))
            )
        return out

    def pair_of(s):
        return xh + (s % 2) * (1 - 2 * xh)

    def valid(s):
        return (s >= 0) & (s <= last) & ((s != 1) | (xh == 1))

    def y_copy(s, d):
        return rdma(
            gst.at[s, (tp + d) % NY], yin.at[s, d - 1], v["yss"].at[s, d - 1], v["yrs"].at[s, d - 1],
            at_y((tp + d) % NY),
        )

    def attend(s):
        g = s // 2
        m = pair_of(s)

        @pl.when(s % 2 == 0)
        def _():
            for cp in x_keys_in(g, near):
                cp.wait_recv()

            @pl.when(g > 0)
            def _():
                for cp in x_keys_in(g, side):
                    cp.wait_recv()
                for i in range(2):
                    for cp in pass_on(g, i):
                        cp.start()
                forward(g + 1)

        @pl.when((s % 2 == 1) & (g > 0))
        def _():
            for i in range(2):
                for cp in passed_in(g, i):
                    cp.wait_recv()

        @pl.when(s == 1)
        def _():
            for xp in (side, far):
                for cp in x_keys_in(0, xp):
                    cp.wait_recv()

        lt = klat[g, pl.ds(2 * m, 2)].reshape(2 * TOK, WIDTH)
        rt = jnp.concatenate([krot[g, 2 * m], krot[g, 2 * m + 1]], axis=1)
        scores = dot(lt, ql[...], 1, 1) + dot(rt, qrd[:, :RDIM], 0, 1)
        weights = jnp.exp(FACTOR * scores - lrow[...])
        k_id = lax.broadcasted_iota(jnp.int32, (2 * TOK, 1), 0)
        k_pos = (2 * m + k_id // TOK) * (2 * TOK) + c * TOK + k_id % TOK
        k_pos = jnp.where(g > 0, -1, k_pos)
        q_id = lax.broadcasted_iota(jnp.int32, (1, ROWS), 1)
        q_pos = (2 * x + q_id // (HEADS * TOK)) * TOK + q_id % TOK
        weights = jnp.where(k_pos <= q_pos, weights, 0.0)
        slopes = dot(lt, gr[...], 1, 1)
        dscores = weights * (slopes - trow[...])
        wl = weights.astype(BF16)
        dl = dscores.astype(BF16)
        grad = FACTOR * dot(dl, ql[...], 1, 0) + dot(wl, gr[...], 1, 0)
        slot = s % SLOTS
        gf[slot, :, :, :WIDTH] = grad[:TOK].reshape(NY, QUART, WIDTH)
        gf[slot, :, :, WIDTH : 2 * WIDTH] = grad[TOK:].reshape(NY, QUART, WIDTH)
        rgrad = FACTOR * dot(dl, qrd[...], 1, 0)
        lane = lax.broadcasted_iota(jnp.int32, (TOK, 128), 1)
        packed = jnp.where(lane < RDIM, rgrad[:TOK], rgrad[TOK:])
        gf[slot, :, :, 2 * WIDTH :] = packed.reshape(NY, QUART, 128)
        gst[s] = gf[slot].astype(BF16)
        for d in (2, 1, 3):
            y_copy(s, d).start()
        mixed[...] += dot(dl, lt, 0, 0)
        rsum[...] += dot(dl, rt, 0, 1)

    def x_copy(g, xp):
        return rdma(
            v["xst"].at[g, xp], v["xin"].at[g, x], v["xss"].at[g, xp], v["xrs"].at[g, x], at_x(xp)
        )

    def x_copy_in(g, xp):
        return rdma(
            v["xst"].at[g, xp], v["xin"].at[g, xp], v["xss"].at[g, xp], v["xrs"].at[g, xp], at_x(xp)
        )

    def reduce_y(s):
        @pl.when(valid(s))
        def _():
            g = s // 2
            m = pair_of(s)
            total = gf[s % SLOTS, tp]
            for d in range(1, NY):
                y_copy(s, d).wait_recv()
                total = total + yin[s, d - 1].astype(F32)
            for b in range(2):
                xp = 2 * m + b
                lat = total[:, b * WIDTH : (b + 1) * WIDTH]
                rot = total[:, 2 * WIDTH :]

                @pl.when(xp == x)
                def _():
                    v["xacc"][g, :, :WIDTH] = lat
                    v["xacc"][g, :, WIDTH:] = rot

                @pl.when(xp != x)
                def _():
                    v["xst"][g, xp, :, :WIDTH] = lat.astype(BF16)
                    v["xst"][g, xp, :, WIDTH:] = rot.astype(BF16)
                    x_copy(g, xp).start()

    def z_copy(g):
        return rdma(
            v["zst"].at[g], v["zin"].at[g], v["zss"].at[g], v["zrs"].at[g], {"sp": sp - 2 * NX * g}
        )

    def reduce_x(s):
        @pl.when((s >= 0) & (s <= last) & (s % 2 == 1))
        def _():
            g = s // 2
            v["facc"][...] = v["xacc"][g]
            for d in range(1, NX):
                xp = (x + d) % NX

                @pl.when((g > 0) | (xp >= 2 * xh))
                def _():
                    x_copy_in(g, xp).wait_recv()
                    v["facc"][...] += v["xin"][g, xp].astype(F32)

            @pl.when(g > 0)
            def _():
                v["zst"][g] = v["facc"][...].astype(BF16)
                z_copy(g).start()

            @pl.when(g == 0)
            def _():
                v["obuf"][tp] = v["facc"][...]

    @pl.loop(0, last + 1)
    def _(s):
        @pl.when(valid(s))
        def _():
            attend(s)

        @pl.when(s == 0)
        def _():
            forward(1)

        @pl.when(s == 0)
        def _():
            met(1)
            greet(2)

        reduce_y(s - 2)
        reduce_x(s - 3)

    half = WIDTH // 2
    mine = pl.ds(pl.multiple_of(half * c, half), half)
    theirs = pl.ds(pl.multiple_of(half * other, half), half)
    my_rows = pl.ds(pl.multiple_of(c * (ROWS // 2), ROWS // 2), ROWS // 2)
    their_rows = pl.ds(pl.multiple_of(other * (ROWS // 2), ROWS // 2), ROWS // 2)
    mix_copy = rdma(mixed.at[:, theirs], v["mrecv"], v["mss"].at[0], v["mrs"].at[0], partner)
    rot_copy = rdma(rsum.at[their_rows], v["rrecv"], v["mss"].at[1], v["mrs"].at[1], partner)
    main_copy = rdma(v["osend"], v["orecv"], v["mss"].at[2], v["mrs"].at[2], partner)
    mix_copy.start()
    rot_copy.start()
    mix_copy.wait_recv()
    ml = v["ml"]
    ml[...] = (mixed[:, mine] + v["mrecv"][...]).astype(BF16)

    def main_part(b, h):
        rows = pl.ds(pl.multiple_of(b * (HEADS * TOK) + h * TOK, TOK), TOK)
        return dot(ml[rows], v["kw"][mine, h * DIM : (h + 1) * DIM], 1, 0)

    for h in range(HEADS):
        cols = slice(h * DIM, (h + 1) * DIM)
        left = jnp.concatenate(
            [ml[b * HEADS * TOK + h * TOK : b * HEADS * TOK + (h + 1) * TOK] for b in range(2)], axis=0
        )
        right = jnp.concatenate([v["qm"][b, :, cols] for b in range(2)], axis=0)
        term = (FACTOR * dot(left, right, 0, 0)).reshape(8, NX, 8, DIM)
        for xp in range(NX):
            v["kf"][xp, :, :, cols] = term[:, xp]
            v["kst"][xp, :, :, cols] = term[:, xp].astype(BF16)

    def kx_copy(xp):
        return rdma(v["kst"].at[xp], v["kxin"].at[x], v["kxs"].at[xp], v["kxr"].at[x], at_x(xp))

    def kx_copy_in(xp):
        return rdma(v["kst"].at[xp], v["kxin"].at[xp], v["kxs"].at[xp], v["kxr"].at[xp], at_x(xp))

    for d in (2, 1, 3):
        kx_copy((x + d) % NX).start()

    for h in range(HEADS):
        v["osend"][:, h * DIM : (h + 1) * DIM] = main_part(other, h)
    main_copy.start()
    reduce_y(last - 1)
    reduce_x(last - 2)
    reduce_y(last)

    total = v["kf"][x]
    for d in range(1, NX):
        xp = (x + d) % NX
        kx_copy_in(xp).wait_recv()
        total = total + v["kxin"][xp].astype(F32)
    total = total.astype(BF16)
    v["kz"][:, 0] = total[:, :PART]
    v["kz"][:, 1] = total[:, PART:]

    def kz_copy(zp, cp):
        return rdma(
            v["kz"].at[zp, cp], v["kzin"].at[z], v["kzs"].at[zp, cp], v["kzr"].at[z],
            {"sp": (8 * c + zp) * 2 * NX + 2 * x + cp},
        )

    met(2)

    @pl.loop(0, 8)
    def _(i):
        zp = (z + i) % 8
        for cp in range(2):
            here = (8 * c + zp == z) & (c == cp)

            @pl.when(jnp.logical_not(here))
            def _():
                kz_copy(zp, cp).start()

            @pl.when(here)
            def _():
                v["kzin"][z] = v["kz"][zp, cp]

    reduce_x(last)
    rot_copy.wait_recv()
    for h in range(HEADS):
        rows = pl.ds(pl.multiple_of(c * (HEADS * TOK) + h * TOK, TOK), TOK)
        o_rot[:, h * RDIM : (h + 1) * RDIM] = FACTOR * (
            rsum[rows] + v["rrecv"][h * TOK : (h + 1) * TOK]
        )
    main_copy.wait_recv()
    for h in range(HEADS):
        cols = slice(h * DIM, (h + 1) * DIM)
        o_main[:, cols] = FACTOR * (main_part(c, h) + v["orecv"][:, cols])

    @pl.loop(1, after + 1)
    def _(d):
        z_copy_in = rdma(
            v["zst"].at[d], v["zin"].at[d], v["zss"].at[d], v["zrs"].at[d], {"sp": sp + 2 * NX * d}
        )
        z_copy_in.wait_recv()
        v["obuf"][tp] += v["zin"][d].astype(F32)

    def ag_copy(d):
        return rdma(
            v["obuf"].at[tp], v["obuf"].at[tp], v["ags"].at[d - 1], v["agr"].at[d - 1],
            at_y((tp + d) % NY),
        )

    for d in (2, 1, 3):
        ag_copy(d).start()

    @pl.loop(0, NZ)
    def _(i):
        @pl.when((i != z) | (c != z // 8))
        def _():
            rdma(
                v["kz"].at[0, 0], v["kzin"].at[i], v["kzs"].at[0, 0], v["kzr"].at[i],
                {"sp": i * 2 * NX + 2 * x + z // 8},
            ).wait_recv()

    total = v["kzin"][0].astype(F32)
    for i in range(1, NZ):
        total = total + v["kzin"][i].astype(F32)
    o_kw[...] = total

    for d in range(1, NY):
        yp = (tp + NY - d) % NY
        rdma(
            v["obuf"].at[yp], v["obuf"].at[yp], v["ags"].at[d - 1], v["agr"].at[d - 1], at_y(yp)
        ).wait_recv()
    out = v["obuf"][...].reshape(TOK, WIDE)
    o_lat[...] = out[:, :WIDTH]
    flip = out[:, WIDTH:].T
    o_krot[...] = jnp.where(x % 2 == 0, flip[:RDIM], flip[RDIM:])

    for n, name in enumerate(shared):
        share(n, name).wait_send()
    @pl.loop(1, zz + 1)
    def _(g):
        for xp in (near, side):
            for cp in x_keys(g, xp):
                cp.wait_send()
        for i in range(2):
            for cp in pass_on(g, i):
                cp.wait_send()

    for xp in (near, side, far):
        @pl.when(xp >= 2 * xh)
        def _():
            for cp in x_keys(0, xp):
                cp.wait_send()

        kx_copy(xp).wait_send()

        @pl.loop(0, zz + 1)
        def _(g):
            @pl.when((g > 0) | (xp // 2 <= xh))
            def _():
                x_copy(g, xp).wait_send()

    @pl.when(after > 0)
    def _():
        @pl.loop(1, zz + 2)
        def _(d):
            for cp in lift(d):
                cp.wait_send()

    @pl.loop(1, zz + 1)
    def _(g):
        z_copy(g).wait_send()

    @pl.loop(0, last + 1)
    def _(s):
        @pl.when(valid(s))
        def _():
            for d in range(1, NY):
                y_copy(s, d).wait_send()

    mix_copy.wait_send()
    rot_copy.wait_send()
    main_copy.wait_send()

    @pl.loop(0, 8)
    def _(zp):
        for cp in range(2):
            @pl.when((8 * c + zp != z) | (c != cp))
            def _():
                kz_copy(zp, cp).wait_send()

    for d in range(1, NY):
        ag_copy(d).wait_send()


def store(*refs):
    *pairs, sem = refs
    count = len(pairs) // 2
    copies = [
        pltpu.make_async_copy(pairs[n], pairs[count + n], sem.at[n]) for n in range(count)
    ]
    for cp in copies:
        cp.start()
    for cp in copies:
        cp.wait()


def per_device(qm, qr, lat, rot, kw, vw, ho, og, logs):
    args = (qm, qr, lat, rot.T, kw, vw, ho, og, logs)
    shapes = (
        (TOK, HEADS * DIM), (TOK, HEADS * RDIM), (TOK, WIDTH), (RDIM, TOK), (PART, HEADS * DIM),
    )
    results = sum(4 * math.prod(s) for s in shapes)
    vmem = pl.BlockSpec(memory_space=pltpu.VMEM)
    hbm = pl.BlockSpec(memory_space=pltpu.HBM)
    held = pl.pallas_call(
        kernel,
        out_shape=[pltpu.VMEM(s, F32) for s in shapes],
        in_specs=[hbm] * len(args),
        out_specs=[vmem] * len(shapes),
        scratch_shapes=list(SCRATCH.values()),
        compiler_params=pltpu.CompilerParams(
            collective_id=0, has_side_effects=True, vmem_limit_bytes=VMEM_BYTES - results - (16 << 10)
        ),
        name="latent_attention_backward",
    )(*args)
    main, rotary, lat_out, rot_out, weight = pl.pallas_call(
        store,
        out_shape=[jax.ShapeDtypeStruct(s, F32) for s in shapes],
        in_specs=[vmem] * len(shapes),
        out_specs=[hbm] * len(shapes),
        scratch_shapes=[DMA((len(shapes),))],
        compiler_params=pltpu.CompilerParams(vmem_limit_bytes=4 << 20),
        name="store_outputs",
    )(*held)
    return main, rotary, lat_out, rot_out.T, weight


def solution(mesh):
    return jax.shard_map(
        per_device,
        mesh=mesh,
        in_specs=(
            P("sp", "tp"),
            P("sp", "tp"),
            P("sp", None),
            P("sp", None),
            P(None, "tp"),
            P(None, "tp"),
            P("sp", "tp"),
            P("sp", "tp"),
            P("tp", "sp"),
        ),
        out_specs=(P("sp", "tp"), P("sp", "tp"), P("sp", None), P("sp", None), P("sp", "tp")),
        check_vma=False,
    )
```
